32 devices in a mesh: ep: 8 (over z, y), tp: 4 (over x, core).
Axes of the slice: x: 2, y: 2, z: 4, core: 2. Of those that a mesh axis runs over, the one named last changes fastest.
Arguments:
- query_latent: bfloat16 [1024, 768], P('ep'), may hold values from -6 to 6
- keyval_latent: bfloat16 [1024, 512], P('ep'), may hold values from -6 to 6
- rotary_key: bfloat16 [1024, 32], P('ep'), may hold values from -6 to 6
- query_gain: float32 [768], replicated, may hold values from 0.3 to 48
- keyval_gain: float32 [512], replicated, may hold values from 0.1 to 1.9
- query_weight: bfloat16 [768, 1536], P(None, 'tp'), may hold values from -0.21875 to 0.21875
- keyval_weight: bfloat16 [512, 2048], P(None, 'tp'), may hold values from -0.25 to 0.25
- output_weight: bfloat16 [1024, 2048], P('tp'), may hold values from -0.1875 to 0.1875
- output_gain: float32 [2048], replicated, may hold values from 0.1 to 1.9
- second_rows: bfloat16 [1024, 2048], P('ep'), may hold values from -6 to 6
- second_gain: float32 [2048], replicated, may hold values from 0.1 to 1.9
- route_ids: int32 [1024, 4], P('ep'), may hold values from 0 to 7, all different within a row; in each aligned block of 128 rows (0 to 127, 128 to 255, ...) at most 128 rows name the same one
- route_weights: float32 [1024, 4], P('ep'), may hold values from 0.1 to 1
- gate_weight: bfloat16 [8, 2048, 1024], P('ep', None, 'tp'), may hold values from -0.125 to 0.125
- up_weight: bfloat16 [8, 2048, 1024], P('ep', None, 'tp'), may hold values from -0.125 to 0.125
- down_weight: bfloat16 [8, 1024, 2048], P('ep', 'tp'), may hold values from -0.1875 to 0.1875
- shared_gate: bfloat16 [2048, 512], P(None, 'tp'), may hold values from -0.125 to 0.125
- shared_up: bfloat16 [2048, 512], P(None, 'tp'), may hold values from -0.125 to 0.125
- shared_down: bfloat16 [512, 2048], P('tp'), may hold values from -0.25 to 0.25
Outputs:
- mixed: bfloat16 [1024, 2048], P(('ep', 'tp'))
- expert_mix: bfloat16 [1024, 2048], P('ep', 'tp')
The draws below stay inside these ranges and needn't reach their ends.
Inputs may be any that keep to these rules, and one draw needn't show every extreme that they name: `route_ids`: each row names 4 different experts. Among the rows of one index of ep (aligned blocks of 128 rows) no expert is named more than 128 times, a bound that some expert reaches in some blocks.
All inputs are finite; a program needn't handle non-finite values.
Results may differ from the reference program's by a relative error of at most 0.023.
The reference program's roundings to bfloat16 on the way count: a program that leaves them out, or rounds other values in their place, can miss the bound.
Values may be sent and summed in bfloat16 or wider, within the bound.
A program may use at most 128 MiB of HBM per device.

```python
import math
import jax
import jax.numpy as jnp
import numpy as np
from jax import lax

D = 2048
HEADS = 16
NOPE = 64
ROPE = 32
VDIM = 64
QLAT = 768
KVLAT = 512
FE = 1024
FS = 512
TOP = 4
TOKB = 128
SEQ = 1024
TOKENS_B = 1024
EXPERTS = 8
CAP = 128
N_EP = 8
N_TP = 4


def draw_query_gain(key, part):
    return jax.random.uniform(key, (QLAT,), jnp.float32, 0.3, 1.7)


def levels(key, extent, cuts, low, largest):
    def one(axis_at, blocks):
        draws = jax.random.uniform(jax.random.fold_in(jax.random.fold_in(key, 6), axis_at), (blocks,), jnp.float32, low / len(cuts), largest / len(cuts))
        return jnp.repeat(jnp.exp(draws), extent[axis_at] // blocks).reshape((-1,) + (1,) * (len(extent) - axis_at - 1))

    loudness = one(*cuts[0])
    for cut in cuts[1:]:
        loudness = loudness * one(*cut)
    return loudness


def assign_block(stream_key, own, number, rows, count, top, bound, lean):
    ranking = jax.random.permutation(stream_key, count)
    packed, common = shares(count, rows * top, bound, lean, True), shares(count, rows * top, bound, lean, False)
    places = jnp.arange(count)

    def named(tallies, turn):
        used = int((tallies > 0).sum())
        fixed = max(1, used // 4)
        moved = fixed + (places - fixed + turn * (used - fixed)) % max(1, count - fixed)
        return jnp.zeros((count,), jnp.int32).at[ranking[jnp.where(places < fixed, places, moved)]].set(jnp.asarray(tallies, jnp.int32))

    tallies = jnp.where(number % 4 == 0, named(packed, number // 4), named(common, number - number // 4 - 1))
    mixed = jax.random.permutation(jax.random.fold_in(own, 3), count)
    source_of, taker = mixed[0:count // 2 * 2:2], mixed[1:count // 2 * 2:2]
    margin = jnp.minimum(tallies[source_of] - 1, bound - tallies[taker]) // 2
    margin = jnp.where((source_of == ranking[0]) | (taker == ranking[0]) | (tallies[taker] == 0), 0, jnp.maximum(margin, 0))
    moved = jax.random.randint(jax.random.fold_in(own, 4), (count // 2,), 0, 1 << 20) % (margin + 1)
    tallies = tallies.at[source_of].add(-moved).at[taker].add(moved)
    labels = jnp.searchsorted(jnp.cumsum(tallies), jnp.arange(rows * top), side="right").astype(jnp.int32)
    table = labels.reshape(top, rows).T
    table = table[jax.random.permutation(jax.random.fold_in(own, 1), rows)]
    turn = jax.random.randint(jax.random.fold_in(own, 2), (rows, 1), 0, top)
    return jnp.take_along_axis(table, (jnp.arange(top)[None, :] + turn) % top, axis=1)


def shares(amount, total, reach, skew, full):
    portions = [(1 << 20) // math.isqrt(grade ** skew) + 1 for grade in range(1, amount + 1)]
    largest = reach if full else min(reach, max(-(-total // amount), total * portions[0] // sum(portions)))
    least = 1 if total - largest >= amount - 1 else 0
    holding, spare = [largest] + [least] * (amount - 1), total - largest - least * (amount - 1)
    while spare > 0:
        movable = [i for i in range(1, amount) if holding[i] < largest] or [i for i in range(1, amount) if holding[i] < reach]
        mass, left = sum([portions[i] for i in movable]), spare
        for i in movable:
            more = min(reach - holding[i], max(1, left * portions[i] // mass), spare)
            holding[i] = holding[i] + more
            spare = spare - more
    return np.array(holding)


def scatter_about(own_key, dims, spread, limit, shards=(), held_as=jnp.bfloat16):
    values = spread * jax.random.normal(own_key, dims, jnp.float32)
    if shards:
        values = values * levels(own_key, dims, shards, -0.22, 0.18)
    return jnp.clip(values, -limit, limit).astype(held_as)


def setup_inputs(seed: int = 0) -> dict:
    seeds = jax.random.split(jax.random.key(seed), 20)
    query_latent = scatter_about(seeds[0], (SEQ, QLAT), 1.0, 6.0, ((0, 8),))
    keyval_latent = scatter_about(seeds[1], (SEQ, KVLAT), 1.0, 6.0, ((0, 8),))
    rotary_key = scatter_about(seeds[2], (SEQ, ROPE), 1.0, 6.0, ((0, 8),))
    query_gain = draw_query_gain(jax.random.fold_in(seeds[19], 71), 0)
    keyval_gain = jnp.clip(1.0 + 0.18 * jax.random.normal(seeds[4], (KVLAT,), jnp.float32), 0.1, 1.9)
    query_weight = scatter_about(seeds[5], (QLAT, HEADS * (NOPE + ROPE)), QLAT ** -0.5, 0.21875, ((1, 4),))
    keyval_weight = scatter_about(seeds[6], (KVLAT, HEADS * (NOPE + VDIM)), KVLAT ** -0.5, 0.25, ((1, 4),))
    output_weight = scatter_about(seeds[7], (HEADS * VDIM, D), (HEADS * VDIM) ** -0.5, 0.1875, ((0, 4),))
    output_gain = jnp.clip(1.0 + 0.18 * jax.random.normal(seeds[8], (D,), jnp.float32), 0.1, 1.9)
    second_rows = scatter_about(seeds[9], (TOKENS_B, D), 1.0, 6.0, ((0, 8),))
    second_gain = jnp.clip(1.0 + 0.18 * jax.random.normal(seeds[10], (D,), jnp.float32), 0.1, 1.9)
    route_ids_keys = jax.random.split(jax.random.fold_in(seeds[11], 1), TOKENS_B // TOKB)
    route_ids_turns = jax.random.permutation(jax.random.fold_in(seeds[11], 3), TOKENS_B // TOKB)
    route_ids = jax.vmap(lambda own, number: assign_block(jax.random.fold_in(seeds[11], 2), own, number, TOKB, EXPERTS, TOP, CAP, 1))(route_ids_keys, route_ids_turns).reshape((TOKENS_B, TOP))
    route_weights = jnp.clip(0.1 + 0.9 * jax.random.uniform(seeds[12], (TOKENS_B, TOP), jnp.float32) ** levels(seeds[12], (TOKENS_B, TOP), ((0, 8),), -0.2, 0.2), 0.1, 1.0)
    gate_weight = scatter_about(seeds[13], (EXPERTS, D, FE), D ** -0.5, 0.125, ((0, 8), (2, 4)))
    up_weight = scatter_about(seeds[14], (EXPERTS, D, FE), D ** -0.5, 0.125, ((0, 8), (2, 4)))
    down_weight = scatter_about(seeds[15], (EXPERTS, FE, D), FE ** -0.5, 0.1875, ((0, 8), (1, 4)))
    shared_gate = scatter_about(seeds[16], (D, FS), D ** -0.5, 0.125, ((1, 4),))
    shared_up = scatter_about(seeds[17], (D, FS), D ** -0.5, 0.125, ((1, 4),))
    shared_down = scatter_about(seeds[18], (FS, D), FS ** -0.5, 0.25, ((0, 4),))
    return {"query_latent": query_latent, "keyval_latent": keyval_latent, "rotary_key": rotary_key, "query_gain": query_gain, "keyval_gain": keyval_gain, "query_weight": query_weight, "keyval_weight": keyval_weight, "output_weight": output_weight, "output_gain": output_gain, "second_rows": second_rows, "second_gain": second_gain, "route_ids": route_ids, "route_weights": route_weights, "gate_weight": gate_weight, "up_weight": up_weight, "down_weight": down_weight, "shared_gate": shared_gate, "shared_up": shared_up, "shared_down": shared_down}


EPS = 1e-06
ROPE_BASE = 10000.0

def rms_scale(values, gain_vec):
    widened = values.astype(jnp.float32)
    normed = widened * lax.rsqrt(lax.optimization_barrier(jnp.mean(widened * widened, -1, keepdims=True)) + EPS)
    return (normed * gain_vec.astype(jnp.float32)).astype(jnp.bfloat16)

def rotate(values, positions):
    half_width = values.shape[-1] // 2
    inverse = 1.0 / ROPE_BASE ** (jnp.arange(half_width, dtype=jnp.float32) * 2.0 / (2 * half_width))
    angles = positions[:, None] * inverse[None, :]
    cosine = jnp.cos(angles)
    sine_vals = jnp.sin(angles)
    if values.ndim == 3:
        cosine = cosine[:, None, :]
        sine_vals = sine_vals[:, None, :]
    first_half = values[..., :half_width]
    second = values[..., half_width:]
    return jnp.concatenate([first_half * cosine - second * sine_vals, first_half * sine_vals + second * cosine], -1)

def round_trip(values):
    return lax.optimization_barrier(values.astype(jnp.bfloat16)).astype(jnp.float32)

def attention_part(query_latent, keyval_latent, rotary_key, query_gain, keyval_gain, query_weight, keyval_weight, output_weight, output_gain):
    positions = jnp.arange(SEQ, dtype=jnp.float32)
    queries = jnp.dot(rms_scale(query_latent, query_gain), query_weight, preferred_element_type=jnp.float32).reshape(SEQ, HEADS, NOPE + ROPE)
    queries = jnp.concatenate([queries[..., :NOPE], rotate(queries[..., NOPE:], positions)], -1).astype(jnp.bfloat16)
    keyvals = jnp.dot(rms_scale(keyval_latent, keyval_gain), keyval_weight, preferred_element_type=jnp.float32).astype(jnp.bfloat16)
    keyvals = keyvals.reshape(SEQ, HEADS, NOPE + VDIM)
    key_rot = rotate(rotary_key.astype(jnp.float32), positions).astype(jnp.bfloat16)
    key_plain = keyvals[..., :NOPE].astype(jnp.float32)
    values_all = keyvals[..., NOPE:].astype(jnp.float32)
    key_rot_wide = key_rot.astype(jnp.float32)
    score_scale = (NOPE + ROPE) ** (-0.5)
    block_rows = math.gcd(SEQ, 512)
    blocks = queries.reshape(SEQ // block_rows, block_rows, HEADS, NOPE + ROPE)

    def attend(query_block):
        query_wide = query_block.astype(jnp.float32)
        scores = jnp.einsum('qhd,khd->hqk', query_wide[..., :NOPE], key_plain)
        scores = (scores + jnp.einsum('qhr,kr->hqk', query_wide[..., NOPE:], key_rot_wide)) * score_scale
        top_score = lax.optimization_barrier(jnp.max(scores, -1, keepdims=True))
        exponent = jnp.exp(scores - top_score)
        denominator = lax.optimization_barrier(jnp.sum(exponent, -1))
        summed = jnp.einsum('hqk,khe->qhe', round_trip(exponent), values_all)
        return (summed / denominator.T[..., None]).astype(jnp.bfloat16)
    attended = lax.map(attend, blocks).reshape(SEQ, HEADS * VDIM)
    group_cols = HEADS * VDIM // N_TP
    mixture = jnp.zeros((SEQ, D), jnp.float32)
    for group_idx in range(N_TP):
        lower = group_idx * group_cols
        partial_value = jnp.dot(attended[:, lower:lower + group_cols], output_weight[lower:lower + group_cols], preferred_element_type=jnp.float32)
        mixture = mixture + round_trip(partial_value)
    return rms_scale(mixture, output_gain)

def grouped_down(hidden, down_mat, width):
    group_width = width // N_TP
    output = jnp.zeros((hidden.shape[0], down_mat.shape[1]), jnp.float32)
    for group_idx in range(N_TP):
        lower = group_idx * group_width
        partial_value = jnp.dot(hidden[:, lower:lower + group_width], down_mat[lower:lower + group_width], preferred_element_type=jnp.float32)
        output = output + round_trip(partial_value)
    return output

def expert_part(second_rows, second_gain, route_ids, route_weights, gate_weight, up_weight, down_weight, shared_gate, shared_up, shared_down):
    normed = rms_scale(second_rows, second_gain)
    padded = jnp.concatenate([normed, jnp.zeros((1, D), jnp.bfloat16)], 0)
    block_ids = route_ids.reshape(N_EP, TOKB * TOP)
    onehot = (block_ids[:, :, None] == jnp.arange(EXPERTS, dtype=jnp.int32)[None, None, :]).astype(jnp.int32)
    slot_rank = lax.optimization_barrier(jnp.sum((jnp.cumsum(onehot, 1) - 1) * onehot, 2))
    owners = (jnp.arange(N_EP * TOKB * TOP, dtype=jnp.int32) // TOP).reshape(N_EP, TOKB * TOP)
    sources = jnp.arange(N_EP, dtype=jnp.int32)[:, None]
    target = ((block_ids * N_EP + sources) * CAP + slot_rank).reshape(-1)
    slot_table = jnp.full((EXPERTS * N_EP * CAP,), N_EP * TOKB, jnp.int32).at[target].set(owners.reshape(-1))

    def run_expert(operands):
        gate_mat, up_mat, down_mat, rows_index = operands
        inputs = padded[rows_index]
        gate_act = jnp.dot(inputs, gate_mat, preferred_element_type=jnp.float32)
        up_act = jnp.dot(inputs, up_mat, preferred_element_type=jnp.float32)
        hidden = (jax.nn.silu(gate_act) * up_act).astype(jnp.bfloat16)
        return grouped_down(hidden, down_mat, FE).astype(jnp.bfloat16)
    expert_out = lax.map(run_expert, (gate_weight, up_weight, down_weight, slot_table.reshape(EXPERTS, N_EP * CAP)))
    expert_out = expert_out.reshape(EXPERTS * N_EP * CAP, D)
    picked = expert_out[target].astype(jnp.float32).reshape(N_EP * TOKB, TOP, D)
    routed = lax.optimization_barrier(jnp.sum(picked * route_weights.astype(jnp.float32)[:, :, None], 1))
    shared_hidden = (jax.nn.silu(jnp.dot(normed, shared_gate, preferred_element_type=jnp.float32)) * jnp.dot(normed, shared_up, preferred_element_type=jnp.float32)).astype(jnp.bfloat16)
    shared_out = grouped_down(shared_hidden, shared_down, FS)
    return (routed + shared_out).astype(jnp.bfloat16)

def reference(query_latent, keyval_latent, rotary_key, query_gain, keyval_gain, query_weight, keyval_weight, output_weight, output_gain, second_rows, second_gain, route_ids, route_weights, gate_weight, up_weight, down_weight, shared_gate, shared_up, shared_down):
    mixed = attention_part(query_latent, keyval_latent, rotary_key, query_gain, keyval_gain, query_weight, keyval_weight, output_weight, output_gain)
    expert_mix = expert_part(second_rows, second_gain, route_ids, route_weights, gate_weight, up_weight, down_weight, shared_gate, shared_up, shared_down)
    return (mixed, expert_mix)
```

```python
import functools
import math

import jax
import jax.numpy as jnp
import numpy as np
from jax import lax
from jax.experimental import pallas as pl
from jax.experimental.pallas import tpu as pltpu
from jax.sharding import PartitionSpec as P

NOPE = 64
ROPE = 32
VDIM = 64


EPS = 1e-06
ROPE_BASE = 10000.0


def rms_scale(values, gain_vec):
    widened = values.astype(jnp.float32)
    normed = widened * lax.rsqrt(jnp.mean(widened * widened, -1, keepdims=True) + EPS)
    return (normed * gain_vec).astype(jnp.bfloat16)


def rotate(values, positions):
    half_width = values.shape[-1] // 2
    inverse = 1.0 / ROPE_BASE ** (
        jnp.arange(half_width, dtype=jnp.float32) * 2.0 / (2 * half_width)
    )
    angles = positions[:, None] * inverse[None, :]
    cosine = jnp.cos(angles)
    sine_vals = jnp.sin(angles)
    if values.ndim == 3:
        cosine = cosine[:, None, :]
        sine_vals = sine_vals[:, None, :]
    first_half = values[..., :half_width]
    second = values[..., half_width:]
    return jnp.concatenate(
        [first_half * cosine - second * sine_vals, first_half * sine_vals + second * cosine], -1
    )


def per_device_slots(
    query_latent,
    keyval_latent,
    rotary_key,
    query_gain,
    keyval_gain,
    query_weight,
    keyval_weight,
    output_weight,
    output_gain,
    second_rows,
    second_gain,
    route_ids,
    route_weights,
    gate_weight,
    up_weight,
    down_weight,
    shared_gate,
    shared_up,
    shared_down,
):
    first_rows = query_latent.shape[0]
    tp_count = lax.axis_size("tp")
    ep_count = lax.axis_size("ep")
    head_count = query_weight.shape[1] // (NOPE + ROPE)
    positions = (lax.axis_index("ep") * first_rows).astype(jnp.float32) + jnp.arange(
        first_rows, dtype=jnp.float32
    )
    queries = jnp.dot(
        rms_scale(query_latent, query_gain), query_weight, preferred_element_type=jnp.float32
    ).reshape(first_rows, head_count, NOPE + ROPE)
    queries = jnp.concatenate(
        [queries[..., :NOPE], rotate(queries[..., NOPE:], positions)], -1
    ).astype(jnp.bfloat16)
    query_plain = queries[..., :NOPE]
    query_turned = queries[..., NOPE:]
    kv_normed = rms_scale(keyval_latent, keyval_gain)
    key_rot = rotate(rotary_key.astype(jnp.float32), positions).astype(jnp.bfloat16)
    score_scale = (NOPE + ROPE) ** (-0.5)

    def attend(carried, pieces):
        highest, denominator, accumulated = carried
        keyval_piece, rot_piece = pieces
        key_count = keyval_piece.shape[0]
        keyval_heads = keyval_piece.reshape(key_count, head_count, NOPE + VDIM)
        scores = jnp.einsum(
            "qhd,khd->hqk",
            query_plain,
            keyval_heads[..., :NOPE],
            preferred_element_type=jnp.float32,
        )
        scores = (
            scores
            + jnp.einsum("qhr,kr->hqk", query_turned, rot_piece, preferred_element_type=jnp.float32)
        ) * score_scale
        new_high = jnp.maximum(highest, jnp.max(scores, -1))
        exponent = jnp.exp(scores - new_high[..., None])
        rescale = jnp.exp(highest - new_high)
        denominator = denominator * rescale + jnp.sum(exponent, -1)
        update = jnp.einsum(
            "hqk,khe->qhe",
            exponent.astype(jnp.bfloat16),
            keyval_heads[..., NOPE:],
            preferred_element_type=jnp.float32,
        )
        accumulated = accumulated * rescale.T[..., None] + update
        return (new_high, denominator, accumulated)

    start_state = (
        jnp.full((head_count, first_rows), -jnp.inf, jnp.float32),
        jnp.zeros((head_count, first_rows), jnp.float32),
        jnp.zeros((first_rows, head_count, VDIM), jnp.float32),
    )
    quarter = first_rows // tp_count
    offset = lax.axis_index("tp") * quarter
    own_latent = lax.dynamic_slice_in_dim(kv_normed, offset, quarter, 0)
    own_rot = lax.dynamic_slice_in_dim(key_rot, offset, quarter, 0)
    all_latent, all_rot = (
        lax.all_gather(own_latent, ("ep", "tp"), axis=0, tiled=True),
        lax.all_gather(own_rot, ("ep", "tp"), axis=0, tiled=True),
    )
    total_keys = all_latent.shape[0]
    key_block = math.gcd(total_keys, 512)
    latent_blocks = all_latent.reshape(total_keys // key_block, key_block, all_latent.shape[1])
    rot_blocks = all_rot.reshape(total_keys // key_block, key_block, all_rot.shape[1])

    def scan_step(carried, block_pair):
        projected = jnp.dot(
            block_pair[0], keyval_weight, preferred_element_type=jnp.float32
        ).astype(jnp.bfloat16)
        return (attend(carried, (projected, block_pair[1])), None)

    final_state, _ = lax.scan(scan_step, start_state, (latent_blocks, rot_blocks))
    denominator = final_state[1]
    accumulated = final_state[2]
    attended = (
        (accumulated / denominator.T[..., None])
        .astype(jnp.bfloat16)
        .reshape(first_rows, head_count * VDIM)
    )
    mixture = lax.psum_scatter(
        jnp.dot(attended, output_weight, preferred_element_type=jnp.float32).astype(jnp.bfloat16),
        "tp",
        scatter_dimension=0,
        tiled=True,
    ).astype(jnp.float32)
    mixed = rms_scale(mixture, output_gain)
    tok_rows = second_rows.shape[0]
    model_width = second_rows.shape[1]
    top_count = route_ids.shape[1]
    local_count = gate_weight.shape[0]
    expert_count = local_count * ep_count
    capacity = max(tp_count, tok_rows * top_count * 2 // expert_count // tp_count * tp_count)
    normed = rms_scale(second_rows, second_gain)
    flat_ids = route_ids.reshape(-1)
    onehot = (flat_ids[:, None] == jnp.arange(expert_count, dtype=jnp.int32)[None, :]).astype(
        jnp.int32
    )
    slot_rank = jnp.sum((jnp.cumsum(onehot, 0) - 1) * onehot, 1)
    owners = jnp.arange(tok_rows * top_count, dtype=jnp.int32) // top_count
    slot_table = (
        jnp.full((expert_count * capacity,), tok_rows, jnp.int32)
        .at[flat_ids * capacity + slot_rank]
        .set(owners)
    )
    padded = jnp.concatenate([normed, jnp.zeros((1, model_width), jnp.bfloat16)], 0)
    outgoing = padded[slot_table].reshape(ep_count, local_count, capacity, model_width)
    weights = route_weights.reshape(-1, 1)
    shared_hidden = (
        jax.nn.silu(jnp.dot(normed, shared_gate, preferred_element_type=jnp.float32))
        * jnp.dot(normed, shared_up, preferred_element_type=jnp.float32)
    ).astype(jnp.bfloat16)
    shared_part = jnp.dot(shared_hidden, shared_down, preferred_element_type=jnp.float32)
    arrived = lax.all_to_all(outgoing, "ep", split_axis=0, concat_axis=0, tiled=True)
    gate_act = jnp.einsum(
        "sicd,idf->sicf", arrived, gate_weight, preferred_element_type=jnp.float32
    )
    up_act = jnp.einsum("sicd,idf->sicf", arrived, up_weight, preferred_element_type=jnp.float32)
    hidden = (jax.nn.silu(gate_act) * up_act).astype(jnp.bfloat16)
    slot_terms = jnp.einsum(
        "sicf,ifd->sicd", hidden, down_weight, preferred_element_type=jnp.float32
    ).reshape(-1, model_width)
    slot_sum, shared_sum = (
        lax.psum_scatter(
            slot_terms.astype(jnp.bfloat16), "tp", scatter_dimension=1, tiled=True
        ).astype(jnp.float32),
        lax.psum_scatter(
            shared_part.astype(jnp.bfloat16), "tp", scatter_dimension=1, tiled=True
        ).astype(jnp.float32),
    )
    column_part = model_width // tp_count
    returned = lax.all_to_all(
        slot_sum.astype(jnp.bfloat16).reshape(ep_count, local_count * capacity, column_part),
        "ep",
        split_axis=0,
        concat_axis=0,
        tiled=True,
    )
    returned = returned.reshape(expert_count * capacity, column_part)
    picked = returned[flat_ids * capacity + slot_rank].astype(jnp.float32) * weights
    routed = jnp.sum(picked.reshape(tok_rows, top_count, column_part), 1)
    expert_mix = (routed + shared_sum).astype(jnp.bfloat16)
    return (mixed, expert_mix)


MESH = pl.DeviceIdType.MESH
LANES = 128


def grid_of(ep_count, tp_count):
    y_count = math.gcd(ep_count, 2)
    k_count = math.gcd(tp_count, 2)
    return (ep_count // y_count, y_count, tp_count // k_count, k_count)


def place_of(dims):
    ep_at, tp_at = lax.axis_index("ep"), lax.axis_index("tp")
    return (
        lax.div(ep_at, dims[1]),
        lax.rem(ep_at, dims[1]),
        lax.div(tp_at, dims[3]),
        lax.rem(tp_at, dims[3]),
    )


def moved(dims, place, dz=0, dy=0, dx=0, dk=0):
    return tuple(
        lax.rem(at + step % size, size) if step % size else at
        for at, step, size in zip(place, (dz, dy, dx, dk), dims)
    )


def device_of(dims, place):
    return (place[0] * dims[1] + place[1], place[2] * dims[3] + place[3])


def block_of(dims, place):
    ep_at, tp_at = device_of(dims, place)
    return ep_at * (dims[2] * dims[3]) + tp_at


def line_order(z_at, count):
    least = jnp.minimum(z_at, count - 1 - z_at)
    order = [z_at]
    for turn in range(1, count):
        far = turn > 2 * least
        step = jnp.where(far, turn - least, (turn + 1) // 2)
        down = jnp.where(far, 2 * z_at >= count, turn % 2 == 1)
        order.append(jnp.where(down, z_at - step, z_at + step))
    return order


LAT, TOK = 0, 1
A, B, C, D = "A", "B", "C", "D"
KA, KB, KC, KD = "kA", "kB", "kC", "kD"
QUERY, PROJECT, ATTEND, HEAD_OUT, MIX_SEND, MIX_DONE = range(10, 16)
EXPERTS, FAR, SIDE_X, SIDE_Y, OWN = range(16, 21)
SCHEDULE = (
    (LAT, C, 0, 0), (TOK, A, 1, 0), (LAT, A, 1, 0), (TOK, A, 2, 0), (TOK, C, 0, 1),
    (TOK, B, 1, 0), (TOK, A, 1, 1), (LAT, A, 2, 0), (TOK, B, 2, 0), (TOK, A, 2, 1),
    (TOK, C, 0, 0), (TOK, B, 1, 1), (TOK, C, 2, 0), (TOK, KC, 0, 0), (EXPERTS, 0, 0),
    (LAT, B, 1, 0), (LAT, C, 2, 0), (TOK, C, 1, 1), (TOK, D, 0, 0), (TOK, D, 0, 1),
    (TOK, C, 2, 1), (TOK, A, 3, 0), (TOK, D, 2, 0), (TOK, D, 1, 1), (LAT, A, 3, 0),
    (LAT, B, 2, 0), (LAT, D, 0, 0), (LAT, KC, 2, 0), (TOK, A, 3, 1), (LAT, C, 1, 0),
    (TOK, KD, 2, 0), (LAT, D, 1, 0), (LAT, D, 2, 0), (LAT, KC, 1, 0), (TOK, B, 2, 1),
    (TOK, D, 2, 1), (TOK, KC, 0, 1), (TOK, KB, 2, 0), (LAT, KD, 2, 0), (TOK, KA, 2, 1), (QUERY,),
    (TOK, KB, 2, 1), (TOK, C, 1, 0), (TOK, KA, 2, 0), (TOK, C, 3, 0), (LAT, KD, 0, 0),
    (LAT, KA, 2, 0), (LAT, KB, 2, 0), (TOK, KC, 2, 0), (TOK, KA, 1, 0), (LAT, KB, 1, 0),
    (TOK, KD, 0, 1), (TOK, KC, 1, 1), (LAT, KD, 1, 0), (TOK, B, 3, 0), (TOK, D, 1, 0),
    (TOK, KA, 3, 1), (TOK, KC, 2, 1), (TOK, KD, 1, 1), (TOK, KD, 2, 1), (LAT, C, 3, 0),
    (EXPERTS, 2, 1), (TOK, C, 3, 1), (EXPERTS, 2, 0), (LAT, KC, 3, 0), (TOK, KC, 1, 0),
    (LAT, B, 3, 0), (FAR, 2), (TOK, KD, 1, 0), (TOK, B, 3, 1), (TOK, KD, 0, 0), (EXPERTS, 1, 1),
    (LAT, KC, 0, 0), (TOK, KC, 3, 1), (FAR, 1), (LAT, D, 3, 0), (TOK, KA, 3, 0), (LAT, KB, 3, 0),
    (TOK, KA, 1, 1), (TOK, D, 3, 1), (TOK, D, 3, 0), (EXPERTS, 0, 1), (TOK, KC, 3, 0),
    (LAT, KA, 3, 0), (SIDE_X, 2), (TOK, KB, 1, 1), (SIDE_Y, 2), (TOK, KD, 3, 0), (TOK, KB, 1, 0),
    (LAT, KA, 1, 0), (EXPERTS, 1, 0), (LAT, KD, 3, 0), (TOK, KD, 3, 1), (TOK, KB, 3, 0),
    (EXPERTS, 3, 1), (FAR, 0), (TOK, KB, 3, 1), (PROJECT,), (ATTEND, 3), (FAR, 3), (SIDE_X, 1),
    (SIDE_Y, 1), (OWN, 2), (EXPERTS, 3, 0), (SIDE_X, 3), (SIDE_Y, 3), (SIDE_Y, 0), (SIDE_X, 0),
    (ATTEND, 0), (ATTEND, 2), (OWN, 1), (ATTEND, 1), (HEAD_OUT,), (OWN, 3), (MIX_SEND,), (OWN, 0),
    (MIX_DONE,),
)
OVER_Y = ((0, 1, 0), (1, 0, 0), (1, 1, 0), (1, 1, 1), (1, 3, 0),)
CHUNKS = (1, 2)
B_OVER_Z = (False, True)
C_OVER_Z = (False, True)
LAST_TURN = max(entry[2] for entry in SCHEDULE if entry[0] in (LAT, TOK))


def relay_way(which, turn, chunk):
    return "y" if (which, turn, chunk) in OVER_Y else "x"


def gather_keys(dims):
    keys = []
    for which in range(2):
        for turn in range(dims[0]):
            names = ["C", "D", "kC", "kD"]
            names += ["F", "B", "kA", "kB"] if turn else ["L", "R", "BL", "BR", "CL", "CR"]
            keys += [(which, n, turn, c) for n in names for c in range(CHUNKS[which])]
    return {key: index for index, key in enumerate(keys)}


def reduce_keys(dims):
    keys = []
    for turn in range(dims[0]):
        keys += [("k", turn, dy, dx) for dy in range(2) for dx in range(2)]
        keys += [("p", turn), ("q", turn), ("x", turn), ("y", turn)]
    keys += [("mk", 0), ("mk", 1), ("mx", 0)]
    return {key: index for index, key in enumerate(keys)}


def reduce_slots(dims):
    slots, sizes = {}, {"half": 0, "mix": 0, "full": 0}
    for key in reduce_keys(dims):
        group = "half" if key[0] in "pq" else ("mix" if key[0][0] == "m" else "full")
        slots[key] = (group, sizes[group])
        sizes[group] += 1
    return slots, sizes


LOADS = (
    "kl",
    "kg",
    "rk",
    "tab",
    "rid",
    "rwt",
    "sr",
    "sg",
    "ql",
    "qg",
    "qw",
    "gate",
    "up",
    "shg",
    "shu",
    "down",
    "shd",
    "kw",
    "ow",
    "og",
)


def layer_kernel(dims, names, *refs):
    ref = dict(zip(names, refs))
    z_count = dims[0]
    me = place_of(dims)
    ep_at = lax.axis_index("ep")
    ep_count = dims[0] * dims[1]
    g_keys, r_keys = gather_keys(dims), reduce_keys(dims)
    slots, _ = reduce_slots(dims)
    zs = line_order(me[0], z_count)
    lat, tok = ref["lat_all"], ref["tok_all"]
    alls = (lat, tok)
    rows = ref["v_sr"].shape[0]
    quarter = rows // (dims[2] * dims[3])
    latent_width = ref["v_kl"].shape[1]
    tile_at = pl.ds(latent_width, LANES)
    head_count = ref["v_qw"].shape[1] // (NOPE + ROPE)
    own_rows = pl.ds(pl.multiple_of(ep_at * rows, rows), rows)
    sent = []

    local = {}
    for number, name in enumerate(LOADS):
        source, target = ref["h_" + name], ref["v_" + name] if "v_" + name in ref else None
        if name == "tab":
            source = source.at[:, own_rows]
        elif name in ("gate", "up", "down"):
            source = source.at[0]
        if name in ("gate", "up"):
            width = source.shape[1]
            target = ref["v_gu"].at[:, pl.ds(width * (name == "up"), width)]
        elif name in ("shg", "shu"):
            width = source.shape[1]
            target = ref["v_sgu"].at[:, pl.ds(width * (name == "shu"), width)]
        local[name] = pltpu.make_async_copy(source, target, ref["load_sem"].at[number])
        local[name].start()

    def loaded(*wanted):
        for name in wanted:
            local[name].wait()

    barrier = pltpu.get_barrier_semaphore()
    peers = [{"dz": dz} for dz in range(1, z_count)] + [{"dy": 1}, {"dx": 1}, {"dk": 1}]
    for peer in peers:
        pl.semaphore_signal(
            barrier,
            inc=1,
            device_id=device_of(dims, moved(dims, me, **peer)),
            device_id_type=MESH,
        )

    def at_place(turn, dy=0, dx=0, dk=0):
        return (zs[turn],) + moved(dims, me, dy=dy, dx=dx, dk=dk)[1:]

    def region(which, place, chunk):
        size = quarter // CHUNKS[which]
        begin = pl.multiple_of(block_of(dims, place) * quarter + chunk * size, size)
        return alls[which].at[pl.ds(begin, size), :]

    def place_from(name, turn):
        return at_place(turn, *{"A": (0, 0), "B": (0, 1), "C": (1, 0), "D": (1, 1)}[name[-1]])[
            :3
        ] + ((moved(dims, me, dk=1) if name[0] == "k" else me)[3],)

    def g_copy(key, place, target):
        at = region(key[0], place, key[3])
        return pltpu.make_async_remote_copy(
            src_ref=at,
            dst_ref=at,
            send_sem=ref["g_send"].at[g_keys[key]],
            recv_sem=ref["g_recv"].at[g_keys[key]],
            device_id=device_of(dims, target),
            device_id_type=MESH,
        )

    def g_send(key, place, **step):
        copy = g_copy(key, place, moved(dims, me, **step))
        copy.start()
        sent.append(copy)

    def line_copy(which, key, place, chunk, target_z):
        at = region(which, place, chunk)
        kind = "BC".find(key[1][0]) + 1
        return pltpu.make_async_remote_copy(
            src_ref=at,
            dst_ref=at,
            send_sem=ref["g_send"].at[g_keys[key]],
            recv_sem=ref["line_recv"].at[which * 3 + kind, place[0], chunk],
            device_id=device_of(dims, (target_z,) + me[1:]),
            device_id_type=MESH,
        )

    line_sent = []

    def line_send(key, place, down):
        target = jnp.where(down, me[0] - 1, me[0] + 1)
        there = (target >= 0) & (target < z_count)
        if key[1][0] in "BC":
            there &= line_order(target, z_count)[1] == me[0]
        copy = line_copy(key[0], key, place, key[3], jnp.where(there, target, me[0]))

        @pl.when(there)
        def _():
            copy.start()

        line_sent.append((there, copy))

    def take(which, name, turn, chunk):
        place = place_from(name, turn)
        if name == "A":
            key = (which, "F", turn, chunk)
            line_copy(which, key, place, chunk, me[0]).wait_recv()
            line_send(key, place, place[0] > me[0])
            if not (turn == 1 and B_OVER_Z[which]):
                g_send((which, "B", turn, chunk), place, dx=1)
            if not (turn == 1 and C_OVER_Z[which]):
                g_send((which, "C", turn, chunk), place, dy=1)
        elif turn == 1 and (name == "B" and B_OVER_Z[which] or name == "C" and C_OVER_Z[which]):
            line_copy(which, (which, name + "L", 0, chunk), place, chunk, me[0]).wait_recv()
        else:
            g_copy((which, name, turn, chunk), place, me).wait_recv()
        if name == "C" and turn == 0 and C_OVER_Z[which]:
            line_send((which, "CL", 0, chunk), place, True)
            line_send((which, "CR", 0, chunk), place, False)
        way = relay_way(which, turn, chunk)
        if name == "B" and turn and way == "y":
            g_send((which, "D", turn, chunk), place, dy=1)
        if name == "C" and way == "x":
            g_send((which, "D", turn, chunk), place, dx=1)
        if name[0] != "k":
            g_send((which, "k" + name, turn, chunk), place, dk=1)

    def rms(values, gain):
        widened = values.astype(jnp.float32)
        scale = lax.rsqrt(jnp.mean(widened * widened, -1, keepdims=True) + EPS)
        return (widened * scale * gain).astype(jnp.bfloat16)

    lane = lax.broadcasted_iota(jnp.int32, (rows, LANES), 1)

    loaded("kl", "kg", "rk", "tab", "rid", "rwt")
    lat[own_rows, pl.ds(0, latent_width)] = rms(ref["v_kl"][...], ref["v_kg"][...].reshape(1, -1))
    half = ROPE // 2
    turned = ref["v_rk"][...].astype(jnp.float32)
    cos_t, sin_t = ref["v_tab"][pl.ds(0, half), :], ref["v_tab"][pl.ds(half, half), :]
    first, second = turned[:half], turned[half:]
    expert = lax.broadcasted_iota(jnp.int32, (ep_count, rows), 0)
    dense = jnp.zeros((ep_count, rows), jnp.float32)
    for choice in range(ref["v_rid"].shape[0]):
        picked = ref["v_rid"][pl.ds(choice, 1), :] == expert
        dense += jnp.where(picked, ref["v_rwt"][pl.ds(choice, 1), :], 0.0)
    high = dense.astype(jnp.bfloat16).astype(jnp.float32)
    upright = jnp.concatenate(
        [
            high,
            dense - high,
            jnp.zeros((NOPE - 2 * ep_count, rows), jnp.float32),
            first * cos_t - second * sin_t,
            first * sin_t + second * cos_t,
            jnp.zeros((LANES - NOPE - ROPE, rows), jnp.float32),
        ],
        0,
    )
    lat[own_rows, tile_at] = upright.T.astype(jnp.bfloat16)

    pl.semaphore_wait(barrier, len(peers))

    def send_own(which):
        for chunk in range(CHUNKS[which]):
            line_send((which, "L", 0, chunk), me, True)
            line_send((which, "R", 0, chunk), me, False)
            g_send((which, "C", 0, chunk), me, dy=1)

    def send_mirror(which):
        for chunk in range(CHUNKS[which]):
            if relay_way(which, 0, chunk) == "y":
                g_send((which, "D", 0, chunk), at_place(0, 0, 1), dy=1)
            if B_OVER_Z[which]:
                line_send((which, "BL", 0, chunk), at_place(0, 0, 1), True)
                line_send((which, "BR", 0, chunk), at_place(0, 0, 1), False)

    send_own(0)
    send_mirror(0)
    loaded("sr", "sg")

    def norm_quarter(place):
        begin = pl.multiple_of(device_of(dims, place)[1] * quarter, quarter)
        target = pl.multiple_of(block_of(dims, place) * quarter, quarter)
        tok[pl.ds(target, quarter), :] = rms(
            ref["v_sr"][pl.ds(begin, quarter), :], ref["v_sg"][...].reshape(1, -1)
        )

    norm_quarter(me)
    send_own(1)
    norm_quarter(moved(dims, me, dx=1))
    send_mirror(1)
    for dx, dk in ((0, 1), (1, 1)):
        norm_quarter(moved(dims, me, dx=dx, dk=dk))

    def make_queries():
        loaded("ql", "qg", "qw")
        product = jnp.dot(
            rms(ref["v_ql"][...], ref["v_qg"][...].reshape(1, -1)),
            ref["v_qw"][...],
            preferred_element_type=jnp.float32,
        )
        blank = jnp.zeros((NOPE, rows), jnp.float32)
        tail = jnp.zeros((LANES - NOPE - ROPE, rows), jnp.float32)
        cos_tile = jnp.concatenate([blank, cos_t, cos_t, tail], 0).T
        sin_tile = jnp.concatenate([blank, -sin_t, sin_t, tail], 0).T
        wide = product.shape[1]
        for head in range(head_count):
            begin = head * (NOPE + ROPE)
            part = pltpu.roll(product, (wide - begin) % wide, 1)[:, :LANES]
            swapped = jnp.where(
                lane < NOPE + half, pltpu.roll(part, LANES - half, 1), pltpu.roll(part, half, 1)
            )
            ref["q_all"][head, :, pl.ds(0, LANES)] = jnp.where(lane < NOPE, part, 0.0).astype(
                jnp.bfloat16
            )
            ref["q_all"][head, :, pl.ds(LANES, LANES)] = (
                part * cos_tile + swapped * sin_tile
            ).astype(jnp.bfloat16)

    outs = [None] * head_count

    def project():
        loaded("kw")
        ref["kv_all"][...] = jnp.dot(
            lat[:, pl.ds(0, latent_width)], ref["v_kw"][...], preferred_element_type=jnp.float32
        ).astype(jnp.bfloat16)

    def attend(head):
        own = ref["kv_all"][:, pl.ds(head * LANES, LANES)]
        keys = jnp.concatenate([own, lat[:, tile_at]], 1)
        scores = lax.dot_general(
            ref["q_all"][head],
            keys,
            (((1,), (1,)), ((), ())),
            preferred_element_type=jnp.float32,
        ) * ((NOPE + ROPE) ** (-0.5))
        exponent = jnp.exp(scores - jnp.max(scores, -1, keepdims=True))
        denominator = jnp.sum(exponent, -1, keepdims=True)
        outs[head] = (
            jnp.dot(exponent.astype(jnp.bfloat16), own, preferred_element_type=jnp.float32)
            / denominator
        )

    def mix_span(dx, dk):
        size = ref["mixed"].shape[0]
        begin = device_of(dims, moved(dims, me, dx=dx, dk=dk))[1] * size
        return pl.ds(pl.multiple_of(begin, size), size)

    stores = {"half": ref["halves"], "mix": ref["mixes"], "full": ref["full"]}

    def r_copy(key, source, target):
        group, index = slots[key]
        return pltpu.make_async_remote_copy(
            src_ref=source,
            dst_ref=stores[group].at[index],
            send_sem=ref["r_send"].at[r_keys[key]],
            recv_sem=ref["r_recv"].at[r_keys[key]],
            device_id=device_of(dims, target),
            device_id_type=MESH,
        )

    def r_send(key, source, **step):
        copy = r_copy(key, source, moved(dims, me, **step))
        copy.start()
        sent.append(copy)

    def landed(key):
        group, index = slots[key]
        at = stores[group].at[index]
        r_copy(key, at, me).wait_recv()
        return at[...].astype(jnp.float32)

    def head_out():
        loaded("ow")
        pairs = [
            jnp.where(lane < VDIM, pltpu.roll(outs[head], VDIM, 1), outs[head + 1])
            for head in range(0, head_count, 2)
        ]
        attended = jnp.concatenate(pairs, 1).astype(jnp.bfloat16)
        ref["head"][...] = jnp.dot(
            attended, ref["v_ow"][...], preferred_element_type=jnp.float32
        ).astype(jnp.bfloat16)
        for dx in (1, 0):
            r_send(("mk", dx), ref["head"].at[mix_span(dx, 1)], dk=1)

    def mix_core(dx):
        return ref["head"][mix_span(dx, 0), :].astype(jnp.float32) + landed(("mk", dx))

    def mix_send():
        ref["mix_sum"][...] = mix_core(1).astype(jnp.bfloat16)
        r_send(("mx", 0), ref["mix_sum"], dx=1)

    def mix_done():
        loaded("og")
        mixture = mix_core(0) + landed(("mx", 0))
        scale = lax.rsqrt(jnp.mean(mixture * mixture, -1, keepdims=True) + EPS)
        ref["mixed"][...] = (mixture * scale * ref["v_og"][...].reshape(1, -1)).astype(jnp.bfloat16)

    parts, sums = ref["parts"], ref["sums"]
    part_width = ref["out"].shape[1]

    def part_of(dz, dy, dx, dk):
        column = device_of(dims, moved(dims, me, dx=dx, dk=dk))[1]
        return parts.at[dz * 2 + dy, column]

    def gated(both):
        width = both.shape[1] // 2
        gate_act, up_act = both[:, :width], both[:, width:]
        return gate_act / (1.0 + jnp.exp(-gate_act)) * up_act

    def experts(dz, dy):
        begin = device_of(dims, at_place(dz, dy))[0] * rows
        span = pl.ds(pl.multiple_of(begin, rows), rows)
        tokens = tok[span, :]
        chosen = (lane == ep_at) | (lane == ep_count + ep_at)
        scale = jnp.sum(
            jnp.where(chosen, lat[span, tile_at].astype(jnp.float32), 0.0), -1, keepdims=True
        )
        if dz == 0 and dy == 0:
            loaded("gate", "up")
        both = jnp.dot(tokens, ref["v_gu"][...], preferred_element_type=jnp.float32)
        hidden = (gated(both) * scale).astype(jnp.bfloat16)
        own = dz == 0 and dy == 0
        if own:
            loaded("shg", "shu", "down", "shd")
            both = jnp.dot(tokens, ref["v_sgu"][...], preferred_element_type=jnp.float32)
            hidden_own = gated(both).astype(jnp.bfloat16)
        for column in range(dims[2] * dims[3]):
            columns = pl.ds(column * part_width, part_width)
            value = jnp.dot(
                hidden, ref["v_down"][:, columns], preferred_element_type=jnp.float32
            )
            if own:
                value += jnp.dot(
                    hidden_own, ref["v_shd"][:, columns], preferred_element_type=jnp.float32
                )
            parts[dz * 2 + dy, column] = value.astype(jnp.bfloat16)
        for dx in (1, 0):
            r_send(("k", dz, dy, dx), part_of(dz, dy, dx, 1), dk=1)

    def core_sum(dz, dy, dx):
        return part_of(dz, dy, dx, 0)[...].astype(jnp.float32) + landed(("k", dz, dy, dx))

    def keep(dz, dy, dx, value):
        index = dz * 4 + dy * 2 + dx
        sums[index] = value.astype(jnp.bfloat16)
        return sums.at[index]

    half_rows = rows // 2

    def finish_far(dz):
        at = keep(dz, 1, 1, core_sum(dz, 1, 1))
        r_send(("p", dz), at.at[pl.ds(0, half_rows)], dy=1)
        r_send(("q", dz), at.at[pl.ds(half_rows, half_rows)], dx=1)

    def finish_side_y(dz):
        value = core_sum(dz, 1, 0)
        value = jnp.concatenate([value[:half_rows], value[half_rows:] + landed(("q", dz))], 0)
        r_send(("y", dz), keep(dz, 1, 0, value), dy=1)

    def finish_side_x(dz):
        value = core_sum(dz, 0, 1)
        value = jnp.concatenate([value[:half_rows] + landed(("p", dz)), value[half_rows:]], 0)
        r_send(("x", dz), keep(dz, 0, 1, value), dx=1)

    final = []

    def z_copy(slot, source, target_z):
        return pltpu.make_async_remote_copy(
            src_ref=source,
            dst_ref=ref["line_parts"].at[slot],
            send_sem=ref["line_send"].at[slot],
            recv_sem=ref["line_done"].at[slot],
            device_id=device_of(dims, (target_z,) + me[1:]),
            device_id_type=MESH,
        )

    def finish_own(dz):
        value = core_sum(dz, 0, 0) + landed(("x", dz)) + landed(("y", dz))
        if dz:
            target = zs[dz]
            slot = lax.rem(me[0] - target + z_count, z_count)
            copy = z_copy(slot, keep(dz, 0, 0, value), target)
            copy.start()
            sent.append(copy)
        else:
            final.append(value)

    def z_landed(turn):
        slot = lax.rem(zs[turn] - me[0] + z_count, z_count)
        at = ref["line_parts"].at[slot]
        z_copy(slot, at, me[0]).wait_recv()
        return at[...].astype(jnp.float32)

    actions = {
        QUERY: make_queries,
        PROJECT: project,
        ATTEND: attend,
        HEAD_OUT: head_out,
        MIX_SEND: mix_send,
        MIX_DONE: mix_done,
        EXPERTS: experts,
        FAR: finish_far,
        SIDE_X: finish_side_x,
        SIDE_Y: finish_side_y,
        OWN: finish_own,
    }
    for entry in SCHEDULE:
        if entry[0] in actions:
            actions[entry[0]](*entry[1:])
        else:
            take(*entry)
    total = final[0]
    for turn in range(1, z_count):
        total = total + z_landed(turn)
    ref["out"][...] = total.astype(jnp.bfloat16)
    for there, copy in line_sent:
        pl.when(there)(copy.wait_send)
    for copy in sent:
        copy.wait_send()


def per_device_fused(ep_count, tp_count, *args):
    (ql, kl, rk, qg, kg, qw, kw, ow, og, sr, sg, rid, rwt, gate, up, down, shg, shu, shd) = args
    dims = grid_of(ep_count, tp_count)
    half = ROPE // 2
    rows, model_width = sr.shape
    angles = (
        np.arange(rows * ep_count, dtype=np.float64)[None, :]
        * ROPE_BASE ** (-np.arange(half, dtype=np.float64) / half)[:, None]
    )
    table = np.concatenate([np.cos(angles), np.sin(angles)], 0).astype(np.float32)
    given = {
        "kl": kl,
        "kg": kg,
        "rk": rk.T,
        "tab": jnp.asarray(table),
        "rid": rid.T,
        "rwt": rwt.T,
        "sr": sr,
        "sg": sg,
        "ql": ql,
        "qg": qg,
        "qw": qw,
        "gate": gate,
        "up": up,
        "shg": shg,
        "shu": shu,
        "down": down,
        "shd": shd,
        "kw": kw,
        "ow": ow,
        "og": og,
    }
    bf16 = jnp.bfloat16
    scratch = {
        "v_" + name: pltpu.VMEM(given[name].shape, given[name].dtype)
        for name in LOADS
        if name not in ("tab", "gate", "up", "down", "shg", "shu")
    }
    hidden = gate.shape[2]
    total = rows * ep_count
    width = model_width // tp_count
    mix_rows = rows // tp_count
    head_count = qw.shape[1] // (NOPE + ROPE)
    _, sizes = reduce_slots(dims)
    scratch |= {
        "v_tab": pltpu.VMEM((ROPE, rows), jnp.float32),
        "v_gu": pltpu.VMEM((model_width, 2 * hidden), bf16),
        "v_sgu": pltpu.VMEM((model_width, 2 * shg.shape[1]), bf16),
        "v_down": pltpu.VMEM(down.shape[1:], bf16),
        "lat_all": pltpu.VMEM((total, kl.shape[1] + LANES), bf16),
        "tok_all": pltpu.VMEM((total, model_width), bf16),
        "kv_all": pltpu.VMEM((total, kw.shape[1]), bf16),
        "q_all": pltpu.VMEM((head_count, rows, 2 * LANES), bf16),
        "head": pltpu.VMEM((rows, model_width), bf16),
        "parts": pltpu.VMEM((ep_count, tp_count, rows, width), bf16),
        "full": pltpu.VMEM((sizes["full"], rows, width), bf16),
        "halves": pltpu.VMEM((sizes["half"], rows // 2, width), bf16),
        "mixes": pltpu.VMEM((sizes["mix"], mix_rows, model_width), bf16),
        "sums": pltpu.VMEM((dims[0] * 4, rows, width), bf16),
        "mix_sum": pltpu.VMEM((mix_rows, model_width), bf16),
        "line_parts": pltpu.VMEM((dims[0], rows, width), bf16),
        "line_send": pltpu.SemaphoreType.DMA((dims[0],)),
        "line_done": pltpu.SemaphoreType.DMA((dims[0],)),
        "line_recv": pltpu.SemaphoreType.DMA((6, dims[0], max(CHUNKS))),
        "load_sem": pltpu.SemaphoreType.DMA((len(LOADS),)),
        "g_send": pltpu.SemaphoreType.DMA((len(gather_keys(dims)),)),
        "g_recv": pltpu.SemaphoreType.DMA((len(gather_keys(dims)),)),
        "r_send": pltpu.SemaphoreType.DMA((len(reduce_keys(dims)),)),
        "r_recv": pltpu.SemaphoreType.DMA((len(reduce_keys(dims)),)),
    }
    names = ["h_" + name for name in LOADS] + ["mixed", "out"] + list(scratch)
    vmem = pl.BlockSpec(memory_space=pltpu.VMEM)
    return pl.pallas_call(
        functools.partial(layer_kernel, dims, names),
        out_shape=[
            pltpu.VMEM((mix_rows, model_width), bf16),
            pltpu.VMEM((rows, width), bf16),
        ],
        in_specs=[pl.BlockSpec(memory_space=pltpu.HBM)] * len(LOADS),
        out_specs=[vmem] * 2,
        scratch_shapes=list(scratch.values()),
        compiler_params=pltpu.CompilerParams(
            collective_id=0, has_side_effects=True, vmem_limit_bytes=56 * 1024 * 1024
        ),
    )(*[given[name] for name in LOADS])


def solution(mesh):
    placed = (
        P("ep", None),
        P("ep", None),
        P("ep", None),
        P(),
        P(),
        P(None, "tp"),
        P(None, "tp"),
        P("tp", None),
        P(),
        P("ep", None),
        P(),
        P("ep", None),
        P("ep", None),
        P("ep", None, "tp"),
        P("ep", None, "tp"),
        P("ep", "tp", None),
        P(None, "tp"),
        P(None, "tp"),
        P("tp", None),
    )

    def per_device(*args):
        ep_count, tp_count = mesh.shape["ep"], mesh.shape["tp"]
        dims = grid_of(ep_count, tp_count)
        tok_rows, top_count = args[11].shape
        expert_count = args[13].shape[0] * ep_count
        capacity = tok_rows * top_count * 2 // expert_count
        head_count = args[5].shape[1] // (NOPE + ROPE)
        if (
            args[13].shape[0] == 1
            and capacity >= tok_rows
            and dims[0] == 1 + LAST_TURN
            and dims[1:] == (2, 2, 2)
            and tok_rows == args[0].shape[0] == LANES
            and head_count % 2 == 0
            and 2 * ep_count <= NOPE
        ):
            return per_device_fused(ep_count, tp_count, *args)
        return per_device_slots(*args)

    return jax.shard_map(
        per_device,
        mesh=mesh,
        in_specs=placed,
        out_specs=(P(("ep", "tp"), None), P("ep", "tp")),
        check_vma=False,
    )
```

```python
import functools
import math

import jax
import jax.numpy as jnp
import numpy as np
from jax import lax
from jax.experimental import pallas as pl
from jax.experimental.pallas import tpu as pltpu
from jax.sharding import PartitionSpec as P

NOPE = 64
ROPE = 32
VDIM = 64


EPS = 1e-06
ROPE_BASE = 10000.0


def rms_scale(values, gain_vec):
    widened = values.astype(jnp.float32)
    normed = widened * lax.rsqrt(jnp.mean(widened * widened, -1, keepdims=True) + EPS)
    return (normed * gain_vec).astype(jnp.bfloat16)


def rotate(values, positions):
    half_width = values.shape[-1] // 2
    inverse = 1.0 / ROPE_BASE ** (
        jnp.arange(half_width, dtype=jnp.float32) * 2.0 / (2 * half_width)
    )
    angles = positions[:, None] * inverse[None, :]
    cosine = jnp.cos(angles)
    sine_vals = jnp.sin(angles)
    if values.ndim == 3:
        cosine = cosine[:, None, :]
        sine_vals = sine_vals[:, None, :]
    first_half = values[..., :half_width]
    second = values[..., half_width:]
    return jnp.concatenate(
        [first_half * cosine - second * sine_vals, first_half * sine_vals + second * cosine], -1
    )


def per_device_slots(
    query_latent,
    keyval_latent,
    rotary_key,
    query_gain,
    keyval_gain,
    query_weight,
    keyval_weight,
    output_weight,
    output_gain,
    second_rows,
    second_gain,
    route_ids,
    route_weights,
    gate_weight,
    up_weight,
    down_weight,
    shared_gate,
    shared_up,
    shared_down,
):
    first_rows = query_latent.shape[0]
    tp_count = lax.axis_size("tp")
    ep_count = lax.axis_size("ep")
    head_count = query_weight.shape[1] // (NOPE + ROPE)
    positions = (lax.axis_index("ep") * first_rows).astype(jnp.float32) + jnp.arange(
        first_rows, dtype=jnp.float32
    )
    queries = jnp.dot(
        rms_scale(query_latent, query_gain), query_weight, preferred_element_type=jnp.float32
    ).reshape(first_rows, head_count, NOPE + ROPE)
    queries = jnp.concatenate(
        [queries[..., :NOPE], rotate(queries[..., NOPE:], positions)], -1
    ).astype(jnp.bfloat16)
    query_plain = queries[..., :NOPE]
    query_turned = queries[..., NOPE:]
    kv_normed = rms_scale(keyval_latent, keyval_gain)
    key_rot = rotate(rotary_key.astype(jnp.float32), positions).astype(jnp.bfloat16)
    score_scale = (NOPE + ROPE) ** (-0.5)

    def attend(carried, pieces):
        highest, denominator, accumulated = carried
        keyval_piece, rot_piece = pieces
        key_count = keyval_piece.shape[0]
        keyval_heads = keyval_piece.reshape(key_count, head_count, NOPE + VDIM)
        scores = jnp.einsum(
            "qhd,khd->hqk",
            query_plain,
            keyval_heads[..., :NOPE],
            preferred_element_type=jnp.float32,
        )
        scores = (
            scores
            + jnp.einsum("qhr,kr->hqk", query_turned, rot_piece, preferred_element_type=jnp.float32)
        ) * score_scale
        new_high = jnp.maximum(highest, jnp.max(scores, -1))
        exponent = jnp.exp(scores - new_high[..., None])
        rescale = jnp.exp(highest - new_high)
        denominator = denominator * rescale + jnp.sum(exponent, -1)
        update = jnp.einsum(
            "hqk,khe->qhe",
            exponent.astype(jnp.bfloat16),
            keyval_heads[..., NOPE:],
            preferred_element_type=jnp.float32,
        )
        accumulated = accumulated * rescale.T[..., None] + update
        return (new_high, denominator, accumulated)

    start_state = (
        jnp.full((head_count, first_rows), -jnp.inf, jnp.float32),
        jnp.zeros((head_count, first_rows), jnp.float32),
        jnp.zeros((first_rows, head_count, VDIM), jnp.float32),
    )
    quarter = first_rows // tp_count
    offset = lax.axis_index("tp") * quarter
    own_latent = lax.dynamic_slice_in_dim(kv_normed, offset, quarter, 0)
    own_rot = lax.dynamic_slice_in_dim(key_rot, offset, quarter, 0)
    all_latent, all_rot = (
        lax.all_gather(own_latent, ("ep", "tp"), axis=0, tiled=True),
        lax.all_gather(own_rot, ("ep", "tp"), axis=0, tiled=True),
    )
    total_keys = all_latent.shape[0]
    key_block = math.gcd(total_keys, 512)
    latent_blocks = all_latent.reshape(total_keys // key_block, key_block, all_latent.shape[1])
    rot_blocks = all_rot.reshape(total_keys // key_block, key_block, all_rot.shape[1])

    def scan_step(carried, block_pair):
        projected = jnp.dot(
            block_pair[0], keyval_weight, preferred_element_type=jnp.float32
        ).astype(jnp.bfloat16)
        return (attend(carried, (projected, block_pair[1])), None)

    final_state, _ = lax.scan(scan_step, start_state, (latent_blocks, rot_blocks))
    denominator = final_state[1]
    accumulated = final_state[2]
    attended = (
        (accumulated / denominator.T[..., None])
        .astype(jnp.bfloat16)
        .reshape(first_rows, head_count * VDIM)
    )
    mixture = lax.psum_scatter(
        jnp.dot(attended, output_weight, preferred_element_type=jnp.float32).astype(jnp.bfloat16),
        "tp",
        scatter_dimension=0,
        tiled=True,
    ).astype(jnp.float32)
    mixed = rms_scale(mixture, output_gain)
    tok_rows = second_rows.shape[0]
    model_width = second_rows.shape[1]
    top_count = route_ids.shape[1]
    local_count = gate_weight.shape[0]
    expert_count = local_count * ep_count
    capacity = max(tp_count, tok_rows * top_count * 2 // expert_count // tp_count * tp_count)
    normed = rms_scale(second_rows, second_gain)
    flat_ids = route_ids.reshape(-1)
    onehot = (flat_ids[:, None] == jnp.arange(expert_count, dtype=jnp.int32)[None, :]).astype(
        jnp.int32
    )
    slot_rank = jnp.sum((jnp.cumsum(onehot, 0) - 1) * onehot, 1)
    owners = jnp.arange(tok_rows * top_count, dtype=jnp.int32) // top_count
    slot_table = (
        jnp.full((expert_count * capacity,), tok_rows, jnp.int32)
        .at[flat_ids * capacity + slot_rank]
        .set(owners)
    )
    padded = jnp.concatenate([normed, jnp.zeros((1, model_width), jnp.bfloat16)], 0)
    outgoing = padded[slot_table].reshape(ep_count, local_count, capacity, model_width)
    weights = route_weights.reshape(-1, 1)
    shared_hidden = (
        jax.nn.silu(jnp.dot(normed, shared_gate, preferred_element_type=jnp.float32))
        * jnp.dot(normed, shared_up, preferred_element_type=jnp.float32)
    ).astype(jnp.bfloat16)
    shared_part = jnp.dot(shared_hidden, shared_down, preferred_element_type=jnp.float32)
    arrived = lax.all_to_all(outgoing, "ep", split_axis=0, concat_axis=0, tiled=True)
    gate_act = jnp.einsum(
        "sicd,idf->sicf", arrived, gate_weight, preferred_element_type=jnp.float32
    )
    up_act = jnp.einsum("sicd,idf->sicf", arrived, up_weight, preferred_element_type=jnp.float32)
    hidden = (jax.nn.silu(gate_act) * up_act).astype(jnp.bfloat16)
    slot_terms = jnp.einsum(
        "sicf,ifd->sicd", hidden, down_weight, preferred_element_type=jnp.float32
    ).reshape(-1, model_width)
    slot_sum, shared_sum = (
        lax.psum_scatter(
            slot_terms.astype(jnp.bfloat16), "tp", scatter_dimension=1, tiled=True
        ).astype(jnp.float32),
        lax.psum_scatter(
            shared_part.astype(jnp.bfloat16), "tp", scatter_dimension=1, tiled=True
        ).astype(jnp.float32),
    )
    column_part = model_width // tp_count
    returned = lax.all_to_all(
        slot_sum.astype(jnp.bfloat16).reshape(ep_count, local_count * capacity, column_part),
        "ep",
        split_axis=0,
        concat_axis=0,
        tiled=True,
    )
    returned = returned.reshape(expert_count * capacity, column_part)
    picked = returned[flat_ids * capacity + slot_rank].astype(jnp.float32) * weights
    routed = jnp.sum(picked.reshape(tok_rows, top_count, column_part), 1)
    expert_mix = (routed + shared_sum).astype(jnp.bfloat16)
    return (mixed, expert_mix)


MESH = pl.DeviceIdType.MESH
LANES = 128


def grid_of(ep_count, tp_count):
    y_count = math.gcd(ep_count, 2)
    k_count = math.gcd(tp_count, 2)
    return (ep_count // y_count, y_count, tp_count // k_count, k_count)


def place_of(dims):
    ep_at, tp_at = lax.axis_index("ep"), lax.axis_index("tp")
    return (
        lax.div(ep_at, dims[1]),
        lax.rem(ep_at, dims[1]),
        lax.div(tp_at, dims[3]),
        lax.rem(tp_at, dims[3]),
    )


def moved(dims, place, dz=0, dy=0, dx=0, dk=0):
    return tuple(
        lax.rem(at + step % size, size) if step % size else at
        for at, step, size in zip(place, (dz, dy, dx, dk), dims)
    )


def device_of(dims, place):
    return (place[0] * dims[1] + place[1], place[2] * dims[3] + place[3])


def block_of(dims, place):
    ep_at, tp_at = device_of(dims, place)
    return ep_at * (dims[2] * dims[3]) + tp_at


def line_order(z_at, count):
    least = jnp.minimum(z_at, count - 1 - z_at)
    order = [z_at]
    for turn in range(1, count):
        far = turn > 2 * least
        step = jnp.where(far, turn - least, (turn + 1) // 2)
        down = jnp.where(far, 2 * z_at >= count, turn % 2 == 1)
        order.append(jnp.where(down, z_at - step, z_at + step))
    return order


LAT, TOK = 0, 1
A, B, C, D = "A", "B", "C", "D"
KA, KB, KC, KD = "kA", "kB", "kC", "kD"
QUERY, PROJECT, ATTEND, HEAD_OUT, MIX_SEND, MIX_DONE = range(10, 16)
EXPERTS, FAR, SIDE_X, SIDE_Y, OWN = range(16, 21)
SCHEDULE = (
    (LAT, A, 1, 0), (LAT, A, 2, 0), (TOK, A, 1, 0), (TOK, A, 2, 0), (LAT, C, 0, 0),
    (EXPERTS, 0, 0), (TOK, A, 1, 1), (TOK, KA, 1, 0), (TOK, A, 2, 1), (TOK, C, 0, 0),
    (TOK, C, 0, 1), (LAT, C, 2, 0), (TOK, B, 2, 0), (LAT, B, 2, 0), (TOK, B, 1, 0),
    (TOK, C, 2, 1), (TOK, A, 3, 1), (TOK, D, 0, 1), (TOK, C, 2, 0), (TOK, KC, 2, 1),
    (LAT, C, 1, 0), (QUERY,), (TOK, D, 2, 0), (TOK, B, 1, 1), (TOK, A, 3, 0), (LAT, D, 2, 0),
    (TOK, KA, 3, 1), (LAT, A, 3, 0), (TOK, C, 1, 0), (TOK, B, 2, 1), (TOK, KC, 2, 0),
    (LAT, KD, 2, 0), (TOK, KB, 1, 0), (TOK, D, 2, 1), (TOK, KC, 1, 0), (LAT, KA, 2, 0),
    (LAT, KC, 2, 0), (TOK, D, 1, 0), (TOK, C, 1, 1), (LAT, KC, 0, 0), (LAT, B, 1, 0),
    (TOK, KC, 0, 0), (TOK, KB, 1, 1), (TOK, KD, 2, 1), (TOK, KC, 0, 1), (TOK, KD, 2, 0),
    (EXPERTS, 2, 1), (LAT, D, 0, 0), (LAT, KA, 1, 0), (TOK, C, 3, 1), (TOK, KB, 2, 1),
    (LAT, KB, 2, 0), (LAT, D, 1, 0), (TOK, KA, 2, 0), (TOK, KC, 1, 1), (TOK, D, 1, 1),
    (TOK, D, 0, 0), (FAR, 2), (TOK, B, 3, 0), (LAT, KD, 1, 0), (TOK, KD, 0, 1), (TOK, KD, 1, 0),
    (LAT, KD, 0, 0), (LAT, KC, 1, 0), (TOK, KD, 1, 1), (EXPERTS, 1, 1), (LAT, C, 3, 0),
    (TOK, KA, 3, 0), (TOK, KD, 0, 0), (TOK, KB, 2, 0), (TOK, KA, 1, 1), (TOK, B, 3, 1),
    (LAT, B, 3, 0), (TOK, KA, 2, 1), (EXPERTS, 2, 0), (TOK, C, 3, 0), (FAR, 1), (TOK, D, 3, 1),
    (LAT, KA, 3, 0), (EXPERTS, 0, 1), (SIDE_Y, 2), (SIDE_X, 2), (LAT, KC, 3, 0), (LAT, KB, 1, 0),
    (TOK, KD, 3, 1), (LAT, D, 3, 0), (TOK, D, 3, 0), (FAR, 0), (LAT, KB, 3, 0), (TOK, KC, 3, 1),
    (TOK, KB, 3, 1), (EXPERTS, 1, 0), (TOK, KC, 3, 0), (TOK, KD, 3, 0), (LAT, KD, 3, 0),
    (TOK, KB, 3, 0), (EXPERTS, 3, 1), (EXPERTS, 3, 0), (FAR, 3), (SIDE_X, 1), (OWN, 2),
    (SIDE_Y, 1), (PROJECT,), (ATTEND, 3), (ATTEND, 2), (SIDE_Y, 3), (SIDE_Y, 0), (SIDE_X, 3),
    (ATTEND, 1), (OWN, 1), (SIDE_X, 0), (ATTEND, 0), (HEAD_OUT,), (OWN, 3), (MIX_SEND,), (OWN, 0),
    (MIX_DONE,),
)
OVER_Y = ((0, 0, 0), (0, 2, 0), (1, 0, 1), (1, 1, 0), (1, 1, 1), (1, 2, 0), (1, 3, 0),)
CHUNKS = (1, 2)
B_OVER_Z = (False, False)
C_OVER_Z = (True, True)
LAST_TURN = max(entry[2] for entry in SCHEDULE if entry[0] in (LAT, TOK))


def relay_way(which, turn, chunk):
    return "y" if (which, turn, chunk) in OVER_Y else "x"


def over_line(which, name, turn):
    return turn and (
        name == A or turn == 1 and (name == B and B_OVER_Z[which] or name == C and C_OVER_Z[which])
    )


def gather_keys(dims):
    keys = []
    for which in range(2):
        for turn in range(dims[0]):
            names = [C, D, KC, KD] + ([A, B, KA, KB] if turn else [])
            keys += [
                (which, name, turn, chunk)
                for name in names
                if not over_line(which, name, turn)
                for chunk in range(CHUNKS[which])
            ]
    return {key: index for index, key in enumerate(keys)}


def line_keys(dims):
    keys = []
    for which in range(2):
        for chunk in range(CHUNKS[which]):
            keys += [(which, A, place, chunk) for place in range(dims[0])]
            keys += [(which, name, 1, chunk) for name in (B, C) if over_line(which, name, 1)]
    return {key: index for index, key in enumerate(keys)}


def reduce_keys(dims):
    keys = []
    for turn in range(dims[0]):
        keys += [("k", turn, dy, dx) for dy in range(2) for dx in range(2)]
        keys += [("p", turn), ("q", turn), ("x", turn), ("y", turn)]
    keys += [("mk", 0), ("mk", 1), ("mx", 0)]
    return {key: index for index, key in enumerate(keys)}


def reduce_slots(dims):
    slots, sizes = {}, {"half": 0, "mix": 0, "full": 0}
    for key in reduce_keys(dims):
        group = "half" if key[0] in "pq" else ("mix" if key[0][0] == "m" else "full")
        slots[key] = (group, sizes[group])
        sizes[group] += 1
    return slots, sizes


LOADS = (
    ("kl", "kg", "rk", "tab", "rid", "rwt"),
    ("sr", "sg"),
    ("ql", "qg", "qw"),
    ("gate", "up"),
    ("shg", "shu", "down", "shd"),
    ("kw",),
    ("ow",),
    ("og",),
)
LOADED = [name for group in LOADS for name in group]


def layer_kernel(dims, names, *refs):
    ref = dict(zip(names, refs))
    z_count = dims[0]
    me = place_of(dims)
    ep_at = lax.axis_index("ep")
    ep_count = dims[0] * dims[1]
    g_keys, l_keys, r_keys = gather_keys(dims), line_keys(dims), reduce_keys(dims)
    slots, _ = reduce_slots(dims)
    zs = line_order(me[0], z_count)
    lat, tok = ref["lat_all"], ref["tok_all"]
    alls = (lat, tok)
    rows = ref["v_sr"].shape[0]
    quarter = rows // (dims[2] * dims[3])
    latent_width = ref["v_kl"].shape[1]
    tile_at = pl.ds(latent_width, LANES)
    head_count = ref["v_qw"].shape[1] // (NOPE + ROPE)
    own_rows = pl.ds(pl.multiple_of(ep_at * rows, rows), rows)
    sent = []

    local = {}
    number_of = {name: number for number, group in enumerate(LOADS) for name in group}
    for name in LOADED:
        source, target = ref["h_" + name], ref["v_" + name] if "v_" + name in ref else None
        if name == "tab":
            source = source.at[:, own_rows]
        elif name in ("gate", "up", "down"):
            source = source.at[0]
        if name in ("gate", "up"):
            width = source.shape[1]
            target = ref["v_gu"].at[:, pl.ds(width * (name == "up"), width)]
        elif name in ("shg", "shu"):
            width = source.shape[1]
            target = ref["v_sgu"].at[:, pl.ds(width * (name == "shu"), width)]
        local[name] = pltpu.make_async_copy(source, target, ref["load_sem"].at[number_of[name]])
        local[name].start()

    def loaded(*wanted):
        for name in wanted:
            local[name].wait()

    barrier = pltpu.get_barrier_semaphore()
    for there, target in ((me[0] > 0, me[0] - 1), (me[0] + 1 < z_count, me[0] + 1)):
        neighbour = (jnp.where(there, target, me[0]),) + me[1:]

        @pl.when(there)
        def _():
            pl.semaphore_signal(
                barrier,
                inc=1,
                device_id=device_of(dims, neighbour),
                device_id_type=MESH,
            )

    sides = ({"dy": 1}, {"dx": 1}, {"dk": 1})
    for side in sides:
        pl.semaphore_signal(
            barrier,
            inc=1,
            device_id=device_of(dims, moved(dims, me, **side)),
            device_id_type=MESH,
        )
    met = len(sides) + jnp.where(me[0] > 0, 1, 0) + jnp.where(me[0] + 1 < z_count, 1, 0)

    def at_place(turn, dy=0, dx=0, dk=0):
        return (zs[turn],) + moved(dims, me, dy=dy, dx=dx, dk=dk)[1:]

    def region(which, place, chunk):
        size = quarter // CHUNKS[which]
        begin = pl.multiple_of(block_of(dims, place) * quarter + chunk * size, size)
        return alls[which].at[pl.ds(begin, size), :]

    def place_from(name, turn):
        return at_place(turn, *{"A": (0, 0), "B": (0, 1), "C": (1, 0), "D": (1, 1)}[name[-1]])[
            :3
        ] + ((moved(dims, me, dk=1) if name[0] == "k" else me)[3],)

    def g_copy(key, place, target):
        at = region(key[0], place, key[3])
        return pltpu.make_async_remote_copy(
            src_ref=at,
            dst_ref=at,
            send_sem=ref["send"].at[0],
            recv_sem=ref["g_recv"].at[g_keys[key]],
            device_id=device_of(dims, target),
            device_id_type=MESH,
        )

    def g_send(key, place, **step):
        copy = g_copy(key, place, moved(dims, me, **step))
        copy.start()
        sent.append(copy)

    def line_copy(key, place, target_z):
        which, name, _, chunk = key
        at = region(which, place, chunk)
        if name == A:
            number = l_keys[(which, A, 0, chunk)] + place[0]
        else:
            number = l_keys[key]
        return pltpu.make_async_remote_copy(
            src_ref=at,
            dst_ref=at,
            send_sem=ref["send"].at[0],
            recv_sem=ref["line_recv"].at[number],
            device_id=device_of(dims, (target_z,) + me[1:]),
            device_id_type=MESH,
        )

    line_sent = []

    def line_send(key, place, down):
        target = jnp.where(down, me[0] - 1, me[0] + 1)
        there = (target >= 0) & (target < z_count)
        if key[1] != A:
            there &= line_order(target, z_count)[1] == me[0]
        copy = line_copy(key, place, jnp.where(there, target, me[0]))

        @pl.when(there)
        def _():
            copy.start()

        line_sent.append((there, copy))

    def both_ways(key, place):
        line_send(key, place, True)
        line_send(key, place, False)

    def take(which, name, turn, chunk):
        place = place_from(name, turn)
        key = (which, name, turn, chunk)
        if over_line(which, name, turn):
            line_copy(key, place, me[0]).wait_recv()
        else:
            g_copy(key, place, me).wait_recv()
        if name == A:
            line_send(key, place, place[0] > me[0])
            if not over_line(which, B, turn):
                g_send((which, B, turn, chunk), place, dx=1)
            if not over_line(which, C, turn):
                g_send((which, C, turn, chunk), place, dy=1)
        if name == C and turn == 0 and over_line(which, C, 1):
            both_ways((which, C, 1, chunk), place)
        way = relay_way(which, turn, chunk)
        if name == "B" and turn and way == "y":
            g_send((which, "D", turn, chunk), place, dy=1)
        if name == "C" and way == "x":
            g_send((which, "D", turn, chunk), place, dx=1)
        if name[0] != "k":
            g_send((which, "k" + name, turn, chunk), place, dk=1)

    def rms(values, gain):
        widened = values.astype(jnp.float32)
        scale = lax.rsqrt(jnp.mean(widened * widened, -1, keepdims=True) + EPS)
        return (widened * scale * gain).astype(jnp.bfloat16)

    lane = lax.broadcasted_iota(jnp.int32, (rows, LANES), 1)

    loaded("kl", "kg", "rk", "tab", "rid", "rwt")
    lat[own_rows, pl.ds(0, latent_width)] = rms(ref["v_kl"][...], ref["v_kg"][...].reshape(1, -1))
    half = ROPE // 2
    turned = ref["v_rk"][...].astype(jnp.float32)
    cos_t, sin_t = ref["v_tab"][pl.ds(0, half), :], ref["v_tab"][pl.ds(half, half), :]
    first, second = turned[:half], turned[half:]
    expert = lax.broadcasted_iota(jnp.int32, (ep_count, rows), 0)
    dense = jnp.zeros((ep_count, rows), jnp.float32)
    for choice in range(ref["v_rid"].shape[0]):
        picked = ref["v_rid"][pl.ds(choice, 1), :] == expert
        dense += jnp.where(picked, ref["v_rwt"][pl.ds(choice, 1), :], 0.0)
    high = dense.astype(jnp.bfloat16).astype(jnp.float32)
    upright = jnp.concatenate(
        [
            high,
            dense - high,
            jnp.zeros((NOPE - 2 * ep_count, rows), jnp.float32),
            first * cos_t - second * sin_t,
            first * sin_t + second * cos_t,
            jnp.zeros((LANES - NOPE - ROPE, rows), jnp.float32),
        ],
        0,
    )
    lat[own_rows, tile_at] = upright.T.astype(jnp.bfloat16)

    pl.semaphore_wait(barrier, met)

    def send_own(which):
        for chunk in range(CHUNKS[which]):
            both_ways((which, A, 0, chunk), me)
            g_send((which, C, 0, chunk), me, dy=1)

    def send_mirror(which):
        mirror = at_place(0, 0, 1)
        for chunk in range(CHUNKS[which]):
            if relay_way(which, 0, chunk) == "y":
                g_send((which, D, 0, chunk), mirror, dy=1)
            if over_line(which, B, 1):
                both_ways((which, B, 1, chunk), mirror)

    send_own(0)
    send_mirror(0)
    loaded("sr", "sg")

    def norm_quarter(place):
        begin = pl.multiple_of(device_of(dims, place)[1] * quarter, quarter)
        target = pl.multiple_of(block_of(dims, place) * quarter, quarter)
        tok[pl.ds(target, quarter), :] = rms(
            ref["v_sr"][pl.ds(begin, quarter), :], ref["v_sg"][...].reshape(1, -1)
        )

    norm_quarter(me)
    send_own(1)
    norm_quarter(moved(dims, me, dx=1))
    send_mirror(1)
    for dx, dk in ((0, 1), (1, 1)):
        norm_quarter(moved(dims, me, dx=dx, dk=dk))

    def make_queries():
        loaded("ql", "qg", "qw")
        product = jnp.dot(
            rms(ref["v_ql"][...], ref["v_qg"][...].reshape(1, -1)),
            ref["v_qw"][...],
            preferred_element_type=jnp.float32,
        )
        blank = jnp.zeros((NOPE, rows), jnp.float32)
        tail = jnp.zeros((LANES - NOPE - ROPE, rows), jnp.float32)
        cos_tile = jnp.concatenate([blank, cos_t, cos_t, tail], 0).T
        sin_tile = jnp.concatenate([blank, -sin_t, sin_t, tail], 0).T
        wide = product.shape[1]
        for head in range(head_count):
            begin = head * (NOPE + ROPE)
            part = pltpu.roll(product, (wide - begin) % wide, 1)[:, :LANES]
            swapped = jnp.where(
                lane < NOPE + half, pltpu.roll(part, LANES - half, 1), pltpu.roll(part, half, 1)
            )
            ref["q_all"][head, :, pl.ds(0, LANES)] = jnp.where(lane < NOPE, part, 0.0).astype(
                jnp.bfloat16
            )
            ref["q_all"][head, :, pl.ds(LANES, LANES)] = (
                part * cos_tile + swapped * sin_tile
            ).astype(jnp.bfloat16)

    outs = [None] * head_count

    def project():
        loaded("kw")
        ref["kv_all"][...] = jnp.dot(
            lat[:, pl.ds(0, latent_width)], ref["v_kw"][...], preferred_element_type=jnp.float32
        ).astype(jnp.bfloat16)

    def attend(head):
        own = ref["kv_all"][:, pl.ds(head * LANES, LANES)]
        keys = jnp.concatenate([own, lat[:, tile_at]], 1)
        scores = lax.dot_general(
            ref["q_all"][head],
            keys,
            (((1,), (1,)), ((), ())),
            preferred_element_type=jnp.float32,
        ) * ((NOPE + ROPE) ** (-0.5))
        exponent = jnp.exp(scores - jnp.max(scores, -1, keepdims=True))
        denominator = jnp.sum(exponent, -1, keepdims=True)
        outs[head] = (
            jnp.dot(exponent.astype(jnp.bfloat16), own, preferred_element_type=jnp.float32)
            / denominator
        )

    def mix_span(dx, dk):
        size = ref["mixed"].shape[0]
        begin = device_of(dims, moved(dims, me, dx=dx, dk=dk))[1] * size
        return pl.ds(pl.multiple_of(begin, size), size)

    stores = {"half": ref["halves"], "mix": ref["mixes"], "full": ref["full"]}

    def r_copy(key, source, target):
        group, index = slots[key]
        return pltpu.make_async_remote_copy(
            src_ref=source,
            dst_ref=stores[group].at[index],
            send_sem=ref["send"].at[0],
            recv_sem=ref["r_recv"].at[r_keys[key]],
            device_id=device_of(dims, target),
            device_id_type=MESH,
        )

    def r_send(key, source, **step):
        copy = r_copy(key, source, moved(dims, me, **step))
        copy.start()
        sent.append(copy)

    def landed(key):
        group, index = slots[key]
        at = stores[group].at[index]
        r_copy(key, at, me).wait_recv()
        return at[...].astype(jnp.float32)

    def head_out():
        loaded("ow")
        pairs = [
            jnp.where(lane < VDIM, pltpu.roll(outs[head], VDIM, 1), outs[head + 1])
            for head in range(0, head_count, 2)
        ]
        attended = jnp.concatenate(pairs, 1).astype(jnp.bfloat16)
        ref["head"][...] = jnp.dot(
            attended, ref["v_ow"][...], preferred_element_type=jnp.float32
        ).astype(jnp.bfloat16)
        for dx in (1, 0):
            r_send(("mk", dx), ref["head"].at[mix_span(dx, 1)], dk=1)

    def mix_core(dx):
        return ref["head"][mix_span(dx, 0), :].astype(jnp.float32) + landed(("mk", dx))

    def mix_send():
        ref["mix_sum"][...] = mix_core(1).astype(jnp.bfloat16)
        r_send(("mx", 0), ref["mix_sum"], dx=1)

    def mix_done():
        loaded("og")
        mixture = mix_core(0) + landed(("mx", 0))
        scale = lax.rsqrt(jnp.mean(mixture * mixture, -1, keepdims=True) + EPS)
        ref["mixed"][...] = (mixture * scale * ref["v_og"][...].reshape(1, -1)).astype(jnp.bfloat16)

    parts, sums = ref["parts"], ref["sums"]
    part_width = ref["out"].shape[1]

    def part_of(dz, dy, dx, dk):
        column = device_of(dims, moved(dims, me, dx=dx, dk=dk))[1]
        return parts.at[dz * 2 + dy, column]

    def gated(both):
        width = both.shape[1] // 2
        gate_act, up_act = both[:, :width], both[:, width:]
        return gate_act / (1.0 + jnp.exp(-gate_act)) * up_act

    def experts(dz, dy):
        begin = device_of(dims, at_place(dz, dy))[0] * rows
        span = pl.ds(pl.multiple_of(begin, rows), rows)
        tokens = tok[span, :]
        chosen = (lane == ep_at) | (lane == ep_count + ep_at)
        scale = jnp.sum(
            jnp.where(chosen, lat[span, tile_at].astype(jnp.float32), 0.0), -1, keepdims=True
        )
        if dz == 0 and dy == 0:
            loaded("gate", "up")
        both = jnp.dot(tokens, ref["v_gu"][...], preferred_element_type=jnp.float32)
        hidden = (gated(both) * scale).astype(jnp.bfloat16)
        own = dz == 0 and dy == 0
        if own:
            loaded("shg", "shu", "down", "shd")
            both = jnp.dot(tokens, ref["v_sgu"][...], preferred_element_type=jnp.float32)
            hidden_own = gated(both).astype(jnp.bfloat16)
        for column in range(dims[2] * dims[3]):
            columns = pl.ds(column * part_width, part_width)
            value = jnp.dot(
                hidden, ref["v_down"][:, columns], preferred_element_type=jnp.float32
            )
            if own:
                value += jnp.dot(
                    hidden_own, ref["v_shd"][:, columns], preferred_element_type=jnp.float32
                )
            parts[dz * 2 + dy, column] = value.astype(jnp.bfloat16)
        for dx in (1, 0):
            r_send(("k", dz, dy, dx), part_of(dz, dy, dx, 1), dk=1)

    def core_sum(dz, dy, dx):
        return part_of(dz, dy, dx, 0)[...].astype(jnp.float32) + landed(("k", dz, dy, dx))

    def keep(dz, dy, dx, value):
        index = dz * 4 + dy * 2 + dx
        sums[index] = value.astype(jnp.bfloat16)
        return sums.at[index]

    half_rows = rows // 2

    def finish_far(dz):
        at = keep(dz, 1, 1, core_sum(dz, 1, 1))
        r_send(("p", dz), at.at[pl.ds(0, half_rows)], dy=1)
        r_send(("q", dz), at.at[pl.ds(half_rows, half_rows)], dx=1)

    def finish_side_y(dz):
        value = core_sum(dz, 1, 0)
        value = jnp.concatenate([value[:half_rows], value[half_rows:] + landed(("q", dz))], 0)
        r_send(("y", dz), keep(dz, 1, 0, value), dy=1)

    def finish_side_x(dz):
        value = core_sum(dz, 0, 1)
        value = jnp.concatenate([value[:half_rows] + landed(("p", dz)), value[half_rows:]], 0)
        r_send(("x", dz), keep(dz, 0, 1, value), dx=1)

    final = []

    def z_copy(slot, source, target_z):
        return pltpu.make_async_remote_copy(
            src_ref=source,
            dst_ref=ref["line_parts"].at[slot],
            send_sem=ref["send"].at[0],
            recv_sem=ref["line_done"].at[slot],
            device_id=device_of(dims, (target_z,) + me[1:]),
            device_id_type=MESH,
        )

    def finish_own(dz):
        value = core_sum(dz, 0, 0) + landed(("x", dz)) + landed(("y", dz))
        if dz:
            target = zs[dz]
            slot = lax.rem(me[0] - target + z_count, z_count)
            copy = z_copy(slot, keep(dz, 0, 0, value), target)
            copy.start()
            sent.append(copy)
        else:
            final.append(value)

    def z_landed(turn):
        slot = lax.rem(zs[turn] - me[0] + z_count, z_count)
        at = ref["line_parts"].at[slot]
        z_copy(slot, at, me[0]).wait_recv()
        return at[...].astype(jnp.float32)

    actions = {
        QUERY: make_queries,
        PROJECT: project,
        ATTEND: attend,
        HEAD_OUT: head_out,
        MIX_SEND: mix_send,
        MIX_DONE: mix_done,
        EXPERTS: experts,
        FAR: finish_far,
        SIDE_X: finish_side_x,
        SIDE_Y: finish_side_y,
        OWN: finish_own,
    }
    for entry in SCHEDULE:
        if entry[0] in actions:
            actions[entry[0]](*entry[1:])
        else:
            take(*entry)
    total = final[0]
    for turn in range(1, z_count):
        total = total + z_landed(turn)
    ref["out"][...] = total.astype(jnp.bfloat16)
    for there, copy in line_sent:
        pl.when(there)(copy.wait_send)
    for copy in sent:
        copy.wait_send()


def per_device_fused(ep_count, tp_count, *args):
    (ql, kl, rk, qg, kg, qw, kw, ow, og, sr, sg, rid, rwt, gate, up, down, shg, shu, shd) = args
    dims = grid_of(ep_count, tp_count)
    half = ROPE // 2
    rows, model_width = sr.shape
    angles = (
        np.arange(rows * ep_count, dtype=np.float64)[None, :]
        * ROPE_BASE ** (-np.arange(half, dtype=np.float64) / half)[:, None]
    )
    table = np.concatenate([np.cos(angles), np.sin(angles)], 0).astype(np.float32)
    given = {
        "kl": kl,
        "kg": kg,
        "rk": rk.T,
        "tab": jnp.asarray(table),
        "rid": rid.T,
        "rwt": rwt.T,
        "sr": sr,
        "sg": sg,
        "ql": ql,
        "qg": qg,
        "qw": qw,
        "gate": gate,
        "up": up,
        "shg": shg,
        "shu": shu,
        "down": down,
        "shd": shd,
        "kw": kw,
        "ow": ow,
        "og": og,
    }
    bf16 = jnp.bfloat16
    scratch = {
        "v_" + name: pltpu.VMEM(given[name].shape, given[name].dtype)
        for name in LOADED
        if name not in ("tab", "gate", "up", "down", "shg", "shu")
    }
    hidden = gate.shape[2]
    total = rows * ep_count
    width = model_width // tp_count
    mix_rows = rows // tp_count
    head_count = qw.shape[1] // (NOPE + ROPE)
    _, sizes = reduce_slots(dims)
    scratch |= {
        "v_tab": pltpu.VMEM((ROPE, rows), jnp.float32),
        "v_gu": pltpu.VMEM((model_width, 2 * hidden), bf16),
        "v_sgu": pltpu.VMEM((model_width, 2 * shg.shape[1]), bf16),
        "v_down": pltpu.VMEM(down.shape[1:], bf16),
        "lat_all": pltpu.VMEM((total, kl.shape[1] + LANES), bf16),
        "tok_all": pltpu.VMEM((total, model_width), bf16),
        "kv_all": pltpu.VMEM((total, kw.shape[1]), bf16),
        "q_all": pltpu.VMEM((head_count, rows, 2 * LANES), bf16),
        "head": pltpu.VMEM((rows, model_width), bf16),
        "parts": pltpu.VMEM((ep_count, tp_count, rows, width), bf16),
        "full": pltpu.VMEM((sizes["full"], rows, width), bf16),
        "halves": pltpu.VMEM((sizes["half"], rows // 2, width), bf16),
        "mixes": pltpu.VMEM((sizes["mix"], mix_rows, model_width), bf16),
        "sums": pltpu.VMEM((dims[0] * 4, rows, width), bf16),
        "mix_sum": pltpu.VMEM((mix_rows, model_width), bf16),
        "line_parts": pltpu.VMEM((dims[0], rows, width), bf16),
        "line_done": pltpu.SemaphoreType.DMA((dims[0],)),
        "line_recv": pltpu.SemaphoreType.DMA((len(line_keys(dims)),)),
        "load_sem": pltpu.SemaphoreType.DMA((len(LOADS),)),
        "send": pltpu.SemaphoreType.DMA((1,)),
        "g_recv": pltpu.SemaphoreType.DMA((len(gather_keys(dims)),)),
        "r_recv": pltpu.SemaphoreType.DMA((len(reduce_keys(dims)),)),
    }
    names = ["h_" + name for name in LOADED] + ["mixed", "out"] + list(scratch)
    vmem = pl.BlockSpec(memory_space=pltpu.VMEM)
    return pl.pallas_call(
        functools.partial(layer_kernel, dims, names),
        out_shape=[
            pltpu.VMEM((mix_rows, model_width), bf16),
            pltpu.VMEM((rows, width), bf16),
        ],
        in_specs=[pl.BlockSpec(memory_space=pltpu.HBM)] * len(LOADED),
        out_specs=[vmem] * 2,
        scratch_shapes=list(scratch.values()),
        compiler_params=pltpu.CompilerParams(
            collective_id=0, has_side_effects=True, vmem_limit_bytes=56 * 1024 * 1024
        ),
    )(*[given[name] for name in LOADED])


def solution(mesh):
    placed = (
        P("ep", None),
        P("ep", None),
        P("ep", None),
        P(),
        P(),
        P(None, "tp"),
        P(None, "tp"),
        P("tp", None),
        P(),
        P("ep", None),
        P(),
        P("ep", None),
        P("ep", None),
        P("ep", None, "tp"),
        P("ep", None, "tp"),
        P("ep", "tp", None),
        P(None, "tp"),
        P(None, "tp"),
        P("tp", None),
    )

    def per_device(*args):
        ep_count, tp_count = mesh.shape["ep"], mesh.shape["tp"]
        dims = grid_of(ep_count, tp_count)
        tok_rows, top_count = args[11].shape
        expert_count = args[13].shape[0] * ep_count
        capacity = tok_rows * top_count * 2 // expert_count
        head_count = args[5].shape[1] // (NOPE + ROPE)
        if (
            args[13].shape[0] == 1
            and capacity >= tok_rows
            and dims[0] == 1 + LAST_TURN
            and dims[1:] == (2, 2, 2)
            and tok_rows == args[0].shape[0] == LANES
            and head_count % 2 == 0
            and 2 * ep_count <= NOPE
        ):
            return per_device_fused(ep_count, tp_count, *args)
        return per_device_slots(*args)

    return jax.shard_map(
        per_device,
        mesh=mesh,
        in_specs=placed,
        out_specs=(P(("ep", "tp"), None), P("ep", "tp")),
        check_vma=False,
    )
```

```python
import functools
import math

import jax
import jax.numpy as jnp
import numpy as np
from jax import lax
from jax.experimental import pallas as pl
from jax.experimental.pallas import tpu as pltpu
from jax.sharding import PartitionSpec as P

NOPE = 64
ROPE = 32
VDIM = 64


EPS = 1e-06
ROPE_BASE = 10000.0


def rms_scale(values, gain_vec):
    widened = values.astype(jnp.float32)
    normed = widened * lax.rsqrt(jnp.mean(widened * widened, -1, keepdims=True) + EPS)
    return (normed * gain_vec).astype(jnp.bfloat16)


def rotate(values, positions):
    half_width = values.shape[-1] // 2
    inverse = 1.0 / ROPE_BASE ** (
        jnp.arange(half_width, dtype=jnp.float32) * 2.0 / (2 * half_width)
    )
    angles = positions[:, None] * inverse[None, :]
    cosine = jnp.cos(angles)
    sine_vals = jnp.sin(angles)
    if values.ndim == 3:
        cosine = cosine[:, None, :]
        sine_vals = sine_vals[:, None, :]
    first_half = values[..., :half_width]
    second = values[..., half_width:]
    return jnp.concatenate(
        [first_half * cosine - second * sine_vals, first_half * sine_vals + second * cosine], -1
    )


def per_device_slots(
    query_latent,
    keyval_latent,
    rotary_key,
    query_gain,
    keyval_gain,
    query_weight,
    keyval_weight,
    output_weight,
    output_gain,
    second_rows,
    second_gain,
    route_ids,
    route_weights,
    gate_weight,
    up_weight,
    down_weight,
    shared_gate,
    shared_up,
    shared_down,
):
    first_rows = query_latent.shape[0]
    tp_count = lax.axis_size("tp")
    ep_count = lax.axis_size("ep")
    head_count = query_weight.shape[1] // (NOPE + ROPE)
    positions = (lax.axis_index("ep") * first_rows).astype(jnp.float32) + jnp.arange(
        first_rows, dtype=jnp.float32
    )
    queries = jnp.dot(
        rms_scale(query_latent, query_gain), query_weight, preferred_element_type=jnp.float32
    ).reshape(first_rows, head_count, NOPE + ROPE)
    queries = jnp.concatenate(
        [queries[..., :NOPE], rotate(queries[..., NOPE:], positions)], -1
    ).astype(jnp.bfloat16)
    query_plain = queries[..., :NOPE]
    query_turned = queries[..., NOPE:]
    kv_normed = rms_scale(keyval_latent, keyval_gain)
    key_rot = rotate(rotary_key.astype(jnp.float32), positions).astype(jnp.bfloat16)
    score_scale = (NOPE + ROPE) ** (-0.5)

    def attend(carried, pieces):
        highest, denominator, accumulated = carried
        keyval_piece, rot_piece = pieces
        key_count = keyval_piece.shape[0]
        keyval_heads = keyval_piece.reshape(key_count, head_count, NOPE + VDIM)
        scores = jnp.einsum(
            "qhd,khd->hqk",
            query_plain,
            keyval_heads[..., :NOPE],
            preferred_element_type=jnp.float32,
        )
        scores = (
            scores
            + jnp.einsum("qhr,kr->hqk", query_turned, rot_piece, preferred_element_type=jnp.float32)
        ) * score_scale
        new_high = jnp.maximum(highest, jnp.max(scores, -1))
        exponent = jnp.exp(scores - new_high[..., None])
        rescale = jnp.exp(highest - new_high)
        denominator = denominator * rescale + jnp.sum(exponent, -1)
        update = jnp.einsum(
            "hqk,khe->qhe",
            exponent.astype(jnp.bfloat16),
            keyval_heads[..., NOPE:],
            preferred_element_type=jnp.float32,
        )
        accumulated = accumulated * rescale.T[..., None] + update
        return (new_high, denominator, accumulated)

    start_state = (
        jnp.full((head_count, first_rows), -jnp.inf, jnp.float32),
        jnp.zeros((head_count, first_rows), jnp.float32),
        jnp.zeros((first_rows, head_count, VDIM), jnp.float32),
    )
    quarter = first_rows // tp_count
    offset = lax.axis_index("tp") * quarter
    own_latent = lax.dynamic_slice_in_dim(kv_normed, offset, quarter, 0)
    own_rot = lax.dynamic_slice_in_dim(key_rot, offset, quarter, 0)
    all_latent, all_rot = (
        lax.all_gather(own_latent, ("ep", "tp"), axis=0, tiled=True),
        lax.all_gather(own_rot, ("ep", "tp"), axis=0, tiled=True),
    )
    total_keys = all_latent.shape[0]
    key_block = math.gcd(total_keys, 512)
    latent_blocks = all_latent.reshape(total_keys // key_block, key_block, all_latent.shape[1])
    rot_blocks = all_rot.reshape(total_keys // key_block, key_block, all_rot.shape[1])

    def scan_step(carried, block_pair):
        projected = jnp.dot(
            block_pair[0], keyval_weight, preferred_element_type=jnp.float32
        ).astype(jnp.bfloat16)
        return (attend(carried, (projected, block_pair[1])), None)

    final_state, _ = lax.scan(scan_step, start_state, (latent_blocks, rot_blocks))
    denominator = final_state[1]
    accumulated = final_state[2]
    attended = (
        (accumulated / denominator.T[..., None])
        .astype(jnp.bfloat16)
        .reshape(first_rows, head_count * VDIM)
    )
    mixture = lax.psum_scatter(
        jnp.dot(attended, output_weight, preferred_element_type=jnp.float32).astype(jnp.bfloat16),
        "tp",
        scatter_dimension=0,
        tiled=True,
    ).astype(jnp.float32)
    mixed = rms_scale(mixture, output_gain)
    tok_rows = second_rows.shape[0]
    model_width = second_rows.shape[1]
    top_count = route_ids.shape[1]
    local_count = gate_weight.shape[0]
    expert_count = local_count * ep_count
    capacity = max(tp_count, tok_rows * top_count * 2 // expert_count // tp_count * tp_count)
    normed = rms_scale(second_rows, second_gain)
    flat_ids = route_ids.reshape(-1)
    onehot = (flat_ids[:, None] == jnp.arange(expert_count, dtype=jnp.int32)[None, :]).astype(
        jnp.int32
    )
    slot_rank = jnp.sum((jnp.cumsum(onehot, 0) - 1) * onehot, 1)
    owners = jnp.arange(tok_rows * top_count, dtype=jnp.int32) // top_count
    slot_table = (
        jnp.full((expert_count * capacity,), tok_rows, jnp.int32)
        .at[flat_ids * capacity + slot_rank]
        .set(owners)
    )
    padded = jnp.concatenate([normed, jnp.zeros((1, model_width), jnp.bfloat16)], 0)
    outgoing = padded[slot_table].reshape(ep_count, local_count, capacity, model_width)
    weights = route_weights.reshape(-1, 1)
    shared_hidden = (
        jax.nn.silu(jnp.dot(normed, shared_gate, preferred_element_type=jnp.float32))
        * jnp.dot(normed, shared_up, preferred_element_type=jnp.float32)
    ).astype(jnp.bfloat16)
    shared_part = jnp.dot(shared_hidden, shared_down, preferred_element_type=jnp.float32)
    arrived = lax.all_to_all(outgoing, "ep", split_axis=0, concat_axis=0, tiled=True)
    gate_act = jnp.einsum(
        "sicd,idf->sicf", arrived, gate_weight, preferred_element_type=jnp.float32
    )
    up_act = jnp.einsum("sicd,idf->sicf", arrived, up_weight, preferred_element_type=jnp.float32)
    hidden = (jax.nn.silu(gate_act) * up_act).astype(jnp.bfloat16)
    slot_terms = jnp.einsum(
        "sicf,ifd->sicd", hidden, down_weight, preferred_element_type=jnp.float32
    ).reshape(-1, model_width)
    slot_sum, shared_sum = (
        lax.psum_scatter(
            slot_terms.astype(jnp.bfloat16), "tp", scatter_dimension=1, tiled=True
        ).astype(jnp.float32),
        lax.psum_scatter(
            shared_part.astype(jnp.bfloat16), "tp", scatter_dimension=1, tiled=True
        ).astype(jnp.float32),
    )
    column_part = model_width // tp_count
    returned = lax.all_to_all(
        slot_sum.astype(jnp.bfloat16).reshape(ep_count, local_count * capacity, column_part),
        "ep",
        split_axis=0,
        concat_axis=0,
        tiled=True,
    )
    returned = returned.reshape(expert_count * capacity, column_part)
    picked = returned[flat_ids * capacity + slot_rank].astype(jnp.float32) * weights
    routed = jnp.sum(picked.reshape(tok_rows, top_count, column_part), 1)
    expert_mix = (routed + shared_sum).astype(jnp.bfloat16)
    return (mixed, expert_mix)


MESH = pl.DeviceIdType.MESH
LANES = 128


def grid_of(ep_count, tp_count):
    y_count = math.gcd(ep_count, 2)
    k_count = math.gcd(tp_count, 2)
    return (ep_count // y_count, y_count, tp_count // k_count, k_count)


def place_of(dims):
    ep_at, tp_at = lax.axis_index("ep"), lax.axis_index("tp")
    return (
        lax.div(ep_at, dims[1]),
        lax.rem(ep_at, dims[1]),
        lax.div(tp_at, dims[3]),
        lax.rem(tp_at, dims[3]),
    )


def moved(dims, place, dz=0, dy=0, dx=0, dk=0):
    return tuple(
        lax.rem(at + step % size, size) if step % size else at
        for at, step, size in zip(place, (dz, dy, dx, dk), dims)
    )


def device_of(dims, place):
    return (place[0] * dims[1] + place[1], place[2] * dims[3] + place[3])


def block_of(dims, place):
    ep_at, tp_at = device_of(dims, place)
    return ep_at * (dims[2] * dims[3]) + tp_at


def line_order(z_at, count):
    least = jnp.minimum(z_at, count - 1 - z_at)
    order = [z_at]
    for turn in range(1, count):
        far = turn > 2 * least
        step = jnp.where(far, turn - least, (turn + 1) // 2)
        down = jnp.where(far, 2 * z_at >= count, turn % 2 == 1)
        order.append(jnp.where(down, z_at - step, z_at + step))
    return order


LAT, TOK = 0, 1
A, B, C, D = "A", "B", "C", "D"
QUERY, PROJECT, ATTEND, HEAD_OUT, MIX_SEND, MIX_DONE = range(10, 16)
EXPERTS, FAR, SIDE_X, SIDE_Y, OWN = range(16, 21)
SCHEDULE = (
    (LAT, A, 1, 0), (LAT, C, 0, 0), (TOK, A, 1, 0), (LAT, A, 2, 0), (TOK, A, 2, 0),
    (TOK, A, 1, 1), (TOK, A, 2, 1), (LAT, A, 3, 0), (TOK, C, 0, 1), (LAT, D, 0, 0),
    (LAT, B, 1, 0), (EXPERTS, 0, 0), (LAT, C, 2, 0), (TOK, C, 0, 0), (TOK, B, 2, 0),
    (LAT, B, 2, 0), (TOK, B, 1, 1), (TOK, C, 2, 1), (TOK, B, 1, 0), (TOK, A, 3, 1),
    (TOK, B, 2, 1), (TOK, C, 2, 0), (TOK, A, 3, 0), (TOK, C, 1, 1), (TOK, D, 2, 0),
    (LAT, D, 2, 0), (TOK, D, 2, 1), (EXPERTS, 2, 0), (LAT, C, 1, 0), (TOK, D, 0, 0),
    (EXPERTS, 2, 1), (TOK, D, 1, 1), (LAT, C, 3, 0), (EXPERTS, 1, 0), (TOK, D, 0, 1),
    (TOK, B, 3, 0), (FAR, 2), (TOK, C, 1, 0), (TOK, B, 3, 1), (QUERY,), (LAT, D, 1, 0),
    (TOK, C, 3, 1), (LAT, B, 3, 0), (SIDE_X, 1, 1), (TOK, D, 1, 0), (LAT, D, 3, 0),
    (EXPERTS, 1, 1), (PROJECT,), (SIDE_X, 2, 1), (SIDE_Y, 2, 1), (TOK, C, 3, 0), (ATTEND, 2),
    (FAR, 1), (TOK, D, 3, 0), (TOK, D, 3, 1), (SIDE_Y, 1, 0), (EXPERTS, 0, 1), (SIDE_X, 2, 0),
    (SIDE_Y, 2, 0), (EXPERTS, 3, 1), (SIDE_X, 0, 1), (OWN, 2, 1), (FAR, 3), (SIDE_Y, 1, 1),
    (ATTEND, 0), (SIDE_X, 1, 0), (ATTEND, 1), (EXPERTS, 3, 0), (FAR, 0), (ATTEND, 3), (HEAD_OUT,),
    (SIDE_Y, 3, 0), (OWN, 2, 0), (OWN, 1, 1), (SIDE_X, 3, 0), (OWN, 1, 0), (SIDE_X, 3, 1),
    (SIDE_Y, 3, 1), (MIX_SEND,), (OWN, 3, 0), (SIDE_Y, 0, 1), (OWN, 3, 1), (SIDE_X, 0, 0),
    (SIDE_Y, 0, 0), (MIX_DONE,), (OWN, 0, 1), (OWN, 0, 0),
)
OVER_Y = ((0, 2, 0), (1, 0, 0), (1, 0, 1), (1, 1, 0), (1, 1, 1), (1, 2, 0), (1, 3, 0),)
CHUNKS = (1, 2)
B_OVER_Z = (False, False)
C_OVER_Z = (True, True)
SIDE_OVER_Z = (True, True)
LAST_TURN = max(entry[2] for entry in SCHEDULE if entry[0] in (LAT, TOK))


def relay_way(which, turn, chunk):
    return "y" if (which, turn, chunk) in OVER_Y else "x"


def over_line(which, name, turn):
    return turn and (
        name == A or turn == 1 and (name == B and B_OVER_Z[which] or name == C and C_OVER_Z[which])
    )


def gather_keys(dims):
    keys = []
    for which in range(2):
        for turn in range(dims[0]):
            names = [C, D] + ([A, B] if turn else [])
            keys += [
                (which, name, turn, chunk)
                for name in names
                if not over_line(which, name, turn)
                for chunk in range(CHUNKS[which])
            ]
    return {key: index for index, key in enumerate(keys)}


def pair_keys(dims):
    keys = [
        (which, name, turn, chunk)
        for which in range(2)
        for turn in range(dims[0])
        for name in ((A, B, C, D) if turn else (C, D))
        for chunk in range(CHUNKS[which])
    ]
    return {key: index for index, key in enumerate(keys)}


def line_keys(dims):
    keys = []
    for which in range(2):
        for chunk in range(CHUNKS[which]):
            keys += [(which, A, place, chunk) for place in range(dims[0])]
            keys += [(which, name, 1, chunk) for name in (B, C) if over_line(which, name, 1)]
    return {key: index for index, key in enumerate(keys)}


def reduce_keys(dims):
    keys = []
    for turn in range(dims[0]):
        keys += [("k", turn, dy, dx) for dy in range(2) for dx in range(2)]
        keys += [("p", turn), ("q", turn)]
        keys += [(side, turn, half) for side in ("x", "y") for half in range(2)]
    keys += [("mk", 0), ("mk", 1), ("mx", 0)]
    return {key: index for index, key in enumerate(keys)}


def reduce_slots(dims):
    slots, sizes = {}, {"half": 0, "mix": 0, "full": 0}
    for key in reduce_keys(dims):
        group = "full" if key[0] == "k" else ("mix" if key[0][0] == "m" else "half")
        slots[key] = (group, sizes[group])
        sizes[group] += 1
    return slots, sizes


LOADS = (
    ("kl", "kg", "rk", "tab", "rid", "rwt"),
    ("sr", "sg"),
    ("ql", "qg", "qw"),
    ("gate", "up"),
    ("shg", "shu", "down", "shd"),
    ("kw",),
    ("ow",),
    ("og",),
)
LOADED = [name for group in LOADS for name in group]


def layer_kernel(dims, names, *refs):
    ref = dict(zip(names, refs))
    z_count = dims[0]
    me = place_of(dims)
    ep_at = lax.axis_index("ep")
    ep_count = dims[0] * dims[1]
    p_keys = pair_keys(dims)
    g_keys, l_keys, r_keys = gather_keys(dims), line_keys(dims), reduce_keys(dims)
    slots, _ = reduce_slots(dims)
    zs = line_order(me[0], z_count)
    lat, tok = ref["lat_all"], ref["tok_all"]
    alls = (lat, tok)
    rows = ref["v_sr"].shape[0]
    quarter = rows // (dims[2] * dims[3])
    latent_width = ref["v_kl"].shape[1]
    tile_at = pl.ds(latent_width, LANES)
    head_count = ref["v_qw"].shape[1] // (NOPE + ROPE)
    own_rows = pl.ds(pl.multiple_of(ep_at * rows, rows), rows)
    sent = []

    local = {}
    number_of = {name: number for number, group in enumerate(LOADS) for name in group}
    for name in LOADED:
        source, target = ref["h_" + name], ref["v_" + name] if "v_" + name in ref else None
        if name == "tab":
            source = source.at[:, own_rows]
        elif name in ("gate", "up", "down"):
            source = source.at[0]
        if name in ("gate", "up"):
            width = source.shape[1]
            target = ref["v_gu"].at[:, pl.ds(width * (name == "up"), width)]
        elif name in ("shg", "shu"):
            width = source.shape[1]
            target = ref["v_sgu"].at[:, pl.ds(width * (name == "shu"), width)]
        local[name] = pltpu.make_async_copy(source, target, ref["load_sem"].at[number_of[name]])
        local[name].start()

    def loaded(*wanted):
        for name in wanted:
            local[name].wait()

    barrier = pltpu.get_barrier_semaphore()
    for there, target in ((me[0] > 0, me[0] - 1), (me[0] + 1 < z_count, me[0] + 1)):
        neighbour = (jnp.where(there, target, me[0]),) + me[1:]

        @pl.when(there)
        def _():
            pl.semaphore_signal(
                barrier,
                inc=1,
                device_id=device_of(dims, neighbour),
                device_id_type=MESH,
            )

    sides = ({"dy": 1}, {"dx": 1}, {"dk": 1})
    for side in sides:
        pl.semaphore_signal(
            barrier,
            inc=1,
            device_id=device_of(dims, moved(dims, me, **side)),
            device_id_type=MESH,
        )
    met = len(sides) + jnp.where(me[0] > 0, 1, 0) + jnp.where(me[0] + 1 < z_count, 1, 0)

    def at_place(turn, dy=0, dx=0, dk=0):
        return (zs[turn],) + moved(dims, me, dy=dy, dx=dx, dk=dk)[1:]

    def region(which, place, chunk):
        size = quarter // CHUNKS[which]
        begin = pl.multiple_of(block_of(dims, place) * quarter + chunk * size, size)
        return alls[which].at[pl.ds(begin, size), :]

    def place_from(name, turn):
        return at_place(turn, int(name in (C, D)), int(name in (B, D)))

    def g_copy(key, place, target):
        at = region(key[0], place, key[3])
        return pltpu.make_async_remote_copy(
            src_ref=at,
            dst_ref=at,
            send_sem=ref["send"].at[0],
            recv_sem=ref["g_recv"].at[g_keys[key]],
            device_id=device_of(dims, target),
            device_id_type=MESH,
        )

    def pair_copy(key, place, target):
        which, name, turn, chunk = key
        at = region(which, place, chunk)
        return pltpu.make_async_remote_copy(
            src_ref=at,
            dst_ref=at,
            send_sem=ref["send"].at[0],
            recv_sem=ref["pair_recv"].at[p_keys[key]],
            device_id=device_of(dims, target),
            device_id_type=MESH,
        )

    paired = set()

    def pair(which, turn, dy):
        if (which, turn, dy) in paired or not (turn or dy):
            return
        paired.add((which, turn, dy))
        for name in (C, D) if dy else (A, B):
            place = place_from(name, turn)
            other = place[:3] + (moved(dims, me, dk=1)[3],)
            for chunk in range(CHUNKS[which]):
                pair_copy((which, name, turn, chunk), other, me).wait_recv()

    def g_send(key, place, **step):
        copy = g_copy(key, place, moved(dims, me, **step))
        copy.start()
        sent.append(copy)

    def line_copy(key, place, target_z):
        which, name, _, chunk = key
        at = region(which, place, chunk)
        if name == A:
            number = l_keys[(which, A, 0, chunk)] + place[0]
        else:
            number = l_keys[key]
        return pltpu.make_async_remote_copy(
            src_ref=at,
            dst_ref=at,
            send_sem=ref["send"].at[0],
            recv_sem=ref["lr"].at[number],
            device_id=device_of(dims, (target_z,) + me[1:]),
            device_id_type=MESH,
        )

    line_sent = []

    def line_send(key, place, down):
        target = jnp.where(down, me[0] - 1, me[0] + 1)
        there = (target >= 0) & (target < z_count)
        if key[1] != A:
            there &= line_order(target, z_count)[1] == me[0]
        copy = line_copy(key, place, jnp.where(there, target, me[0]))

        @pl.when(there)
        def _():
            copy.start()

        line_sent.append((there, copy))

    def both_ways(key, place):
        line_send(key, place, True)
        line_send(key, place, False)

    def take(which, name, turn, chunk):
        place = place_from(name, turn)
        key = (which, name, turn, chunk)
        if over_line(which, name, turn):
            line_copy(key, place, me[0]).wait_recv()
        else:
            g_copy(key, place, me).wait_recv()
        if name == A:
            line_send(key, place, place[0] > me[0])
            if not over_line(which, B, turn):
                g_send((which, B, turn, chunk), place, dx=1)
            if not over_line(which, C, turn):
                g_send((which, C, turn, chunk), place, dy=1)
        if name == C and turn == 0 and over_line(which, C, 1):
            both_ways((which, C, 1, chunk), place)
        way = relay_way(which, turn, chunk)
        if name == "B" and turn and way == "y":
            g_send((which, "D", turn, chunk), place, dy=1)
        if name == "C" and way == "x":
            g_send((which, "D", turn, chunk), place, dx=1)
        copy = pair_copy(key, place, moved(dims, me, dk=1))
        copy.start()
        sent.append(copy)

    def rms(values, gain):
        widened = values.astype(jnp.float32)
        scale = lax.rsqrt(jnp.mean(widened * widened, -1, keepdims=True) + EPS)
        return (widened * scale * gain).astype(jnp.bfloat16)

    lane = lax.broadcasted_iota(jnp.int32, (rows, LANES), 1)

    loaded("kl", "kg", "rk", "tab", "rid", "rwt")
    lat[own_rows, pl.ds(0, latent_width)] = rms(ref["v_kl"][...], ref["v_kg"][...].reshape(1, -1))
    half = ROPE // 2
    turned = ref["v_rk"][...].astype(jnp.float32)
    cos_t, sin_t = ref["v_tab"][pl.ds(0, half), :], ref["v_tab"][pl.ds(half, half), :]
    first, second = turned[:half], turned[half:]
    expert = lax.broadcasted_iota(jnp.int32, (ep_count, rows), 0)
    dense = jnp.zeros((ep_count, rows), jnp.float32)
    for choice in range(ref["v_rid"].shape[0]):
        picked = ref["v_rid"][pl.ds(choice, 1), :] == expert
        dense += jnp.where(picked, ref["v_rwt"][pl.ds(choice, 1), :], 0.0)
    high = dense.astype(jnp.bfloat16).astype(jnp.float32)
    upright = jnp.concatenate(
        [
            high,
            dense - high,
            jnp.zeros((NOPE - 2 * ep_count, rows), jnp.float32),
            first * cos_t - second * sin_t,
            first * sin_t + second * cos_t,
            jnp.zeros((LANES - NOPE - ROPE, rows), jnp.float32),
        ],
        0,
    )
    lat[own_rows, tile_at] = upright.T.astype(jnp.bfloat16)

    pl.semaphore_wait(barrier, met)

    def send_own(which):
        for chunk in range(CHUNKS[which]):
            both_ways((which, A, 0, chunk), me)
            g_send((which, C, 0, chunk), me, dy=1)

    def send_mirror(which):
        mirror = at_place(0, 0, 1)
        for chunk in range(CHUNKS[which]):
            if relay_way(which, 0, chunk) == "y":
                g_send((which, D, 0, chunk), mirror, dy=1)
            if over_line(which, B, 1):
                both_ways((which, B, 1, chunk), mirror)

    send_own(0)
    send_mirror(0)
    loaded("sr", "sg")

    def norm_quarter(place):
        begin = pl.multiple_of(device_of(dims, place)[1] * quarter, quarter)
        target = pl.multiple_of(block_of(dims, place) * quarter, quarter)
        tok[pl.ds(target, quarter), :] = rms(
            ref["v_sr"][pl.ds(begin, quarter), :], ref["v_sg"][...].reshape(1, -1)
        )

    norm_quarter(me)
    send_own(1)
    norm_quarter(moved(dims, me, dx=1))
    send_mirror(1)
    for dx, dk in ((0, 1), (1, 1)):
        norm_quarter(moved(dims, me, dx=dx, dk=dk))

    def make_queries():
        loaded("ql", "qg", "qw")
        product = jnp.dot(
            rms(ref["v_ql"][...], ref["v_qg"][...].reshape(1, -1)),
            ref["v_qw"][...],
            preferred_element_type=jnp.float32,
        )
        blank = jnp.zeros((NOPE, rows), jnp.float32)
        tail = jnp.zeros((LANES - NOPE - ROPE, rows), jnp.float32)
        cos_tile = jnp.concatenate([blank, cos_t, cos_t, tail], 0).T
        sin_tile = jnp.concatenate([blank, -sin_t, sin_t, tail], 0).T
        wide = product.shape[1]
        for head in range(head_count):
            begin = head * (NOPE + ROPE)
            part = pltpu.roll(product, (wide - begin) % wide, 1)[:, :LANES]
            swapped = jnp.where(
                lane < NOPE + half, pltpu.roll(part, LANES - half, 1), pltpu.roll(part, half, 1)
            )
            ref["q_all"][head, :, pl.ds(0, LANES)] = jnp.where(lane < NOPE, part, 0.0).astype(
                jnp.bfloat16
            )
            ref["q_all"][head, :, pl.ds(LANES, LANES)] = (
                part * cos_tile + swapped * sin_tile
            ).astype(jnp.bfloat16)

    outs = [None] * head_count

    def project():
        loaded("kw")
        for turn in range(z_count):
            pair(LAT, turn, 0)
            pair(LAT, turn, 1)
        ref["kv_all"][...] = jnp.dot(
            lat[:, pl.ds(0, latent_width)], ref["v_kw"][...], preferred_element_type=jnp.float32
        ).astype(jnp.bfloat16)

    def attend(head):
        own = ref["kv_all"][:, pl.ds(head * LANES, LANES)]
        keys = jnp.concatenate([own, lat[:, tile_at]], 1)
        scores = lax.dot_general(
            ref["q_all"][head],
            keys,
            (((1,), (1,)), ((), ())),
            preferred_element_type=jnp.float32,
        ) * ((NOPE + ROPE) ** (-0.5))
        exponent = jnp.exp(scores - jnp.max(scores, -1, keepdims=True))
        denominator = jnp.sum(exponent, -1, keepdims=True)
        outs[head] = (
            jnp.dot(exponent.astype(jnp.bfloat16), own, preferred_element_type=jnp.float32)
            / denominator
        )

    def mix_span(dx, dk):
        size = ref["mixed"].shape[0]
        begin = device_of(dims, moved(dims, me, dx=dx, dk=dk))[1] * size
        return pl.ds(pl.multiple_of(begin, size), size)

    stores = {"half": ref["halves"], "mix": ref["mixes"], "full": ref["full"]}

    def r_copy(key, source, target):
        group, index = slots[key]
        return pltpu.make_async_remote_copy(
            src_ref=source,
            dst_ref=stores[group].at[index],
            send_sem=ref["send"].at[0],
            recv_sem=ref["r_recv"].at[r_keys[key]],
            device_id=device_of(dims, target),
            device_id_type=MESH,
        )

    def r_send(key, source, **step):
        copy = r_copy(key, source, moved(dims, me, **step))
        copy.start()
        sent.append(copy)

    def landed(key):
        group, index = slots[key]
        at = stores[group].at[index]
        r_copy(key, at, me).wait_recv()
        return at[...].astype(jnp.float32)

    def head_out():
        loaded("ow")
        pairs = [
            jnp.where(lane < VDIM, pltpu.roll(outs[head], VDIM, 1), outs[head + 1])
            for head in range(0, head_count, 2)
        ]
        attended = jnp.concatenate(pairs, 1).astype(jnp.bfloat16)
        ref["head"][...] = jnp.dot(
            attended, ref["v_ow"][...], preferred_element_type=jnp.float32
        ).astype(jnp.bfloat16)
        for dx in (1, 0):
            r_send(("mk", dx), ref["head"].at[mix_span(dx, 1)], dk=1)

    def mix_core(dx):
        return ref["head"][mix_span(dx, 0), :].astype(jnp.float32) + landed(("mk", dx))

    def mix_send():
        ref["mix_sum"][...] = mix_core(1).astype(jnp.bfloat16)
        r_send(("mx", 0), ref["mix_sum"], dx=1)

    def mix_done():
        loaded("og")
        mixture = mix_core(0) + landed(("mx", 0))
        scale = lax.rsqrt(jnp.mean(mixture * mixture, -1, keepdims=True) + EPS)
        ref["mixed"][...] = (mixture * scale * ref["v_og"][...].reshape(1, -1)).astype(jnp.bfloat16)

    parts, sums = ref["parts"], ref["sums"]
    part_width = ref["out"].shape[1]

    def part_of(dz, dy, dx, dk):
        column = device_of(dims, moved(dims, me, dx=dx, dk=dk))[1]
        return parts.at[dz * 2 + dy, column]

    def gated(both):
        width = both.shape[1] // 2
        gate_act, up_act = both[:, :width], both[:, width:]
        return gate_act / (1.0 + jnp.exp(-gate_act)) * up_act

    def experts(dz, dy):
        pair(LAT, dz, dy)
        pair(TOK, dz, dy)
        begin = device_of(dims, at_place(dz, dy))[0] * rows
        span = pl.ds(pl.multiple_of(begin, rows), rows)
        tokens = tok[span, :]
        chosen = (lane == ep_at) | (lane == ep_count + ep_at)
        scale = jnp.sum(
            jnp.where(chosen, lat[span, tile_at].astype(jnp.float32), 0.0), -1, keepdims=True
        )
        if dz == 0 and dy == 0:
            loaded("gate", "up")
        both = jnp.dot(tokens, ref["v_gu"][...], preferred_element_type=jnp.float32)
        hidden = (gated(both) * scale).astype(jnp.bfloat16)
        own = dz == 0 and dy == 0
        if own:
            loaded("shg", "shu", "down", "shd")
            both = jnp.dot(tokens, ref["v_sgu"][...], preferred_element_type=jnp.float32)
            hidden_own = gated(both).astype(jnp.bfloat16)
        for column in range(dims[2] * dims[3]):
            columns = pl.ds(column * part_width, part_width)
            value = jnp.dot(
                hidden, ref["v_down"][:, columns], preferred_element_type=jnp.float32
            )
            if own:
                value += jnp.dot(
                    hidden_own, ref["v_shd"][:, columns], preferred_element_type=jnp.float32
                )
            parts[dz * 2 + dy, column] = value.astype(jnp.bfloat16)
        for dx in (1, 0):
            r_send(("k", dz, dy, dx), part_of(dz, dy, dx, 1), dk=1)

    half_rows = rows // 2
    both_cores = set()

    def core_sum(dz, dy, dx, half):
        key = ("k", dz, dy, dx)
        at = stores["full"].at[slots[key][1]]
        if key not in both_cores:
            both_cores.add(key)
            r_copy(key, at, me).wait_recv()
        span = pl.ds(half * half_rows, half_rows)
        mine = part_of(dz, dy, dx, 0)[span, :].astype(jnp.float32)
        return mine + at[span, :].astype(jnp.float32)

    def keep(dz, dy, dx, half, value):
        at = sums.at[dz * 4 + dy * 2 + dx, pl.ds(half * half_rows, half_rows)]
        at[...] = value.astype(jnp.bfloat16)
        return at

    def finish_far(dz):
        r_send(("p", dz), keep(dz, 1, 1, 0, core_sum(dz, 1, 1, 0)), dy=1)
        r_send(("q", dz), keep(dz, 1, 1, 1, core_sum(dz, 1, 1, 1)), dx=1)

    def side_copy(side, over, half, source, target_z):
        slot = side * 4 + over * 2 + half
        return pltpu.make_async_remote_copy(
            src_ref=source,
            dst_ref=ref["sp"].at[slot],
            send_sem=ref["send"].at[0],
            recv_sem=ref["sd"].at[slot],
            device_id=device_of(dims, (target_z,) + me[1:]),
            device_id_type=MESH,
        )

    def side_send(over, half, source):
        side = jnp.where(zs[1] > me[0], 0, 1)
        copy = side_copy(side, over, half, source, zs[1])
        copy.start()
        sent.append(copy)

    def with_sides(over, half, value):
        ref["ss"][...] = value
        for side, source in enumerate((me[0] - 1, me[0] + 1)):
            there = (source >= 0) & (source < z_count)
            there &= line_order(source, z_count)[1] == me[0]

            @pl.when(there)
            def _():
                at = ref["sp"].at[side * 4 + over * 2 + half]
                side_copy(side, over, half, at, me[0]).wait_recv()
                ref["ss"][...] += at[...].astype(jnp.float32)

        return ref["ss"][...]

    def finish_side_y(dz, half):
        value = core_sum(dz, 1, 0, half)
        if half:
            value += landed(("q", dz))
        if dz == 0 and SIDE_OVER_Z[1]:
            value = with_sides(1, half, value)
        at = keep(dz, 1, 0, half, value)
        if dz == 1 and SIDE_OVER_Z[1]:
            side_send(1, half, at)
        else:
            r_send(("y", dz, half), at, dy=1)

    def finish_side_x(dz, half):
        value = core_sum(dz, 0, 1, half)
        if not half:
            value += landed(("p", dz))
        if dz == 0 and SIDE_OVER_Z[0]:
            value = with_sides(0, half, value)
        at = keep(dz, 0, 1, half, value)
        if dz == 1 and SIDE_OVER_Z[0]:
            side_send(0, half, at)
        else:
            r_send(("x", dz, half), at, dx=1)

    def z_copy(slot, half, source, target_z):
        return pltpu.make_async_remote_copy(
            src_ref=source,
            dst_ref=ref["lp"].at[slot * 2 + half],
            send_sem=ref["send"].at[0],
            recv_sem=ref["ld"].at[slot * 2 + half],
            device_id=device_of(dims, (target_z,) + me[1:]),
            device_id_type=MESH,
        )

    def finish_own(dz, half):
        value = core_sum(dz, 0, 0, half)
        for over, side in enumerate(("x", "y")):
            if not (dz == 1 and SIDE_OVER_Z[over]):
                value += landed((side, dz, half))
        if dz:
            target = zs[dz]
            slot = lax.rem(me[0] - target + z_count, z_count)
            copy = z_copy(slot, half, keep(dz, 0, 0, half, value), target)
            copy.start()
            sent.append(copy)
        else:
            ref["os"][half] = value

    def z_landed(turn, half):
        slot = lax.rem(zs[turn] - me[0] + z_count, z_count)
        at = ref["lp"].at[slot * 2 + half]
        z_copy(slot, half, at, me[0]).wait_recv()
        return at[...].astype(jnp.float32)

    actions = {
        QUERY: make_queries,
        PROJECT: project,
        ATTEND: attend,
        HEAD_OUT: head_out,
        MIX_SEND: mix_send,
        MIX_DONE: mix_done,
        EXPERTS: experts,
        FAR: finish_far,
        SIDE_X: finish_side_x,
        SIDE_Y: finish_side_y,
        OWN: finish_own,
    }
    for entry in SCHEDULE:
        if entry[0] in actions:
            actions[entry[0]](*entry[1:])
        else:
            take(*entry)
    for half in range(2):
        total = ref["os"][half]
        for turn in range(1, z_count):
            total = total + z_landed(turn, half)
        ref["out"][pl.ds(half * half_rows, half_rows), :] = total.astype(jnp.bfloat16)
    for there, copy in line_sent:
        pl.when(there)(copy.wait_send)
    for copy in sent:
        copy.wait_send()


def per_device_fused(ep_count, tp_count, *args):
    (ql, kl, rk, qg, kg, qw, kw, ow, og, sr, sg, rid, rwt, gate, up, down, shg, shu, shd) = args
    dims = grid_of(ep_count, tp_count)
    half = ROPE // 2
    rows, model_width = sr.shape
    angles = (
        np.arange(rows * ep_count, dtype=np.float64)[None, :]
        * ROPE_BASE ** (-np.arange(half, dtype=np.float64) / half)[:, None]
    )
    table = np.concatenate([np.cos(angles), np.sin(angles)], 0).astype(np.float32)
    given = {
        "kl": kl,
        "kg": kg,
        "rk": rk.T,
        "tab": jnp.asarray(table),
        "rid": rid.T,
        "rwt": rwt.T,
        "sr": sr,
        "sg": sg,
        "ql": ql,
        "qg": qg,
        "qw": qw,
        "gate": gate,
        "up": up,
        "shg": shg,
        "shu": shu,
        "down": down,
        "shd": shd,
        "kw": kw,
        "ow": ow,
        "og": og,
    }
    bf16 = jnp.bfloat16
    scratch = {
        "v_" + name: pltpu.VMEM(given[name].shape, given[name].dtype)
        for name in LOADED
        if name not in ("tab", "gate", "up", "down", "shg", "shu")
    }
    hidden = gate.shape[2]
    total = rows * ep_count
    width = model_width // tp_count
    mix_rows = rows // tp_count
    head_count = qw.shape[1] // (NOPE + ROPE)
    _, sizes = reduce_slots(dims)
    scratch |= {
        "v_tab": pltpu.VMEM((ROPE, rows), jnp.float32),
        "v_gu": pltpu.VMEM((model_width, 2 * hidden), bf16),
        "v_sgu": pltpu.VMEM((model_width, 2 * shg.shape[1]), bf16),
        "v_down": pltpu.VMEM(down.shape[1:], bf16),
        "lat_all": pltpu.VMEM((total, kl.shape[1] + LANES), bf16),
        "tok_all": pltpu.VMEM((total, model_width), bf16),
        "kv_all": pltpu.VMEM((total, kw.shape[1]), bf16),
        "q_all": pltpu.VMEM((head_count, rows, 2 * LANES), bf16),
        "head": pltpu.VMEM((rows, model_width), bf16),
        "parts": pltpu.VMEM((ep_count, tp_count, rows, width), bf16),
        "full": pltpu.VMEM((sizes["full"], rows, width), bf16),
        "halves": pltpu.VMEM((sizes["half"], rows // 2, width), bf16),
        "mixes": pltpu.VMEM((sizes["mix"], mix_rows, model_width), bf16),
        "sums": pltpu.VMEM((dims[0] * 4, rows, width), bf16),
        "mix_sum": pltpu.VMEM((mix_rows, model_width), bf16),
        "lp": pltpu.VMEM((2 * dims[0], rows // 2, width), bf16),
        "sp": pltpu.VMEM((8, rows // 2, width), bf16),
        "ss": pltpu.VMEM((rows // 2, width), jnp.float32),
        "sd": pltpu.SemaphoreType.DMA((8,)),
        "os": pltpu.VMEM((2, rows // 2, width), jnp.float32),
        "ld": pltpu.SemaphoreType.DMA((2 * dims[0],)),
        "lr": pltpu.SemaphoreType.DMA((len(line_keys(dims)),)),
        "load_sem": pltpu.SemaphoreType.DMA((len(LOADS),)),
        "send": pltpu.SemaphoreType.DMA((1,)),
        "pair_recv": pltpu.SemaphoreType.DMA((len(pair_keys(dims)),)),
        "g_recv": pltpu.SemaphoreType.DMA((len(gather_keys(dims)),)),
        "r_recv": pltpu.SemaphoreType.DMA((len(reduce_keys(dims)),)),
    }
    names = ["h_" + name for name in LOADED] + ["mixed", "out"] + list(scratch)
    vmem = pl.BlockSpec(memory_space=pltpu.VMEM)
    return pl.pallas_call(
        functools.partial(layer_kernel, dims, names),
        out_shape=[
            pltpu.VMEM((mix_rows, model_width), bf16),
            pltpu.VMEM((rows, width), bf16),
        ],
        in_specs=[pl.BlockSpec(memory_space=pltpu.HBM)] * len(LOADED),
        out_specs=[vmem] * 2,
        scratch_shapes=list(scratch.values()),
        compiler_params=pltpu.CompilerParams(
            collective_id=0, has_side_effects=True, vmem_limit_bytes=56 * 1024 * 1024
        ),
    )(*[given[name] for name in LOADED])


def solution(mesh):
    placed = (
        P("ep", None),
        P("ep", None),
        P("ep", None),
        P(),
        P(),
        P(None, "tp"),
        P(None, "tp"),
        P("tp", None),
        P(),
        P("ep", None),
        P(),
        P("ep", None),
        P("ep", None),
        P("ep", None, "tp"),
        P("ep", None, "tp"),
        P("ep", "tp", None),
        P(None, "tp"),
        P(None, "tp"),
        P("tp", None),
    )

    def per_device(*args):
        ep_count, tp_count = mesh.shape["ep"], mesh.shape["tp"]
        dims = grid_of(ep_count, tp_count)
        tok_rows, top_count = args[11].shape
        expert_count = args[13].shape[0] * ep_count
        capacity = tok_rows * top_count * 2 // expert_count
        head_count = args[5].shape[1] // (NOPE + ROPE)
        if (
            args[13].shape[0] == 1
            and capacity >= tok_rows
            and dims[0] == 1 + LAST_TURN
            and dims[1:] == (2, 2, 2)
            and tok_rows == args[0].shape[0] == LANES
            and head_count % 2 == 0
            and 2 * ep_count <= NOPE
        ):
            return per_device_fused(ep_count, tp_count, *args)
        return per_device_slots(*args)

    return jax.shard_map(
        per_device,
        mesh=mesh,
        in_specs=placed,
        out_specs=(P(("ep", "tp"), None), P("ep", "tp")),
        check_vma=False,
    )
```
